128 devices in a mesh: fs: 16 (over z, y), tp: 8 (over x, core).
Axes of the slice: x: 4, y: 4, z: 4, core: 2. Of those that a mesh axis runs over, the one named last changes fastest.
Arguments:
- inputs: bfloat16 [8192, 3072], P('fs', 'tp'), may hold values from -6 to 6
- cotangent: bfloat16 [8192, 3072], P('fs', 'tp'), may hold values from -6 to 6
- pre_norm: bfloat16 [8192, 3072], P('fs', 'tp'), may hold values from -28 to 28, as said below
- gate_pre: bfloat16 [8192, 5632], P('fs', 'tp'), may hold values from -8 to 8
- value_pre: bfloat16 [8192, 5632], P('fs', 'tp'), may hold values from -6 to 6
- gate_weight: bfloat16 [3072, 5632], P('fs', 'tp'), may hold values from -0.109375 to 0.109375
- value_weight: bfloat16 [3072, 5632], P('fs', 'tp'), may hold values from -0.109375 to 0.109375
- down_weight: bfloat16 [5632, 3072], P('tp', 'fs'), may hold values from -0.078125 to 0.078125
- conv_taps: float32 [3, 5632], P(None, 'tp'), may hold values from -3.5 to 3.5
- norm_gain: float32 [3072], P('tp'), may hold values from 0.1 to 1.9
Outputs:
- grad_input: bfloat16 [8192, 3072], P('fs', 'tp')
- grad_gate: float32 [3072, 5632], P('fs', 'tp')
- grad_value: float32 [3072, 5632], P('fs', 'tp')
- grad_down: float32 [5632, 3072], P('tp', 'fs')
- grad_taps: float32 [3, 5632], P(None, 'tp')
- grad_gain: float32 [3072], P('tp')
The draws below stay inside these ranges and needn't reach their ends.
Inputs may be any that keep to these rules, and one draw needn't show every extreme that they name: `pre_norm`: every entry has magnitude 0.075 or more.
All inputs are finite; a program needn't handle non-finite values.
Results may differ from the reference program's by a relative error of at most 0.014.
Values may be sent and summed in bfloat16 or wider, within the bound.
A program may use at most 128 MiB of HBM per device.

```python
import jax
import jax.numpy as jnp
from jax import lax

D = 3072
FF = 5632
SEQ = 128
TOKENS = 8192
N_TP = 8


def draw_pre_norm(key, part):
    base = jax.random.fold_in(key, 11)
    first, second, third, fourth = jax.random.split(base, 4)
    blocks = jnp.exp(jax.random.uniform(first, (8,), jnp.float32, jnp.log(0.3), jnp.log(3.0)))
    column_scale = jnp.repeat(blocks, D // 8)
    magnitude = 0.5 + jnp.minimum(jnp.abs(jax.random.normal(second, (TOKENS, D), jnp.float32)), 4.0)
    signs = jnp.where(jax.random.bernoulli(third, 0.5, (TOKENS, D)), 1.0, -1.0)
    row_scale = jnp.exp(jax.random.uniform(fourth, (TOKENS, 1), jnp.float32, -0.7, 0.7))
    return (signs * magnitude * column_scale[None, :] * row_scale).astype(jnp.bfloat16)


def strengthened(entries, own_key, source, target, parts, factor):
    owner, partner = [(jnp.arange(entries.shape[axis_at]) // (entries.shape[axis_at] // parts)).reshape([-1 if axis == axis_at else 1 for axis in range(entries.ndim)]) for axis_at in (source, target)]
    chosen = jax.random.permutation(own_key, parts)[partner]
    strong = (owner == chosen) | (owner == (partner + parts // 2) % parts)
    return jnp.where(strong, factor * entries, entries)


def block_scale(key, dims, cuts, low, top_value):
    level, own = 1.0, jax.random.fold_in(key, 6)
    for position, parts in cuts:
        draws = jnp.exp(jax.random.uniform(jax.random.fold_in(own, position), (parts,), jnp.float32, low / len(cuts), top_value / len(cuts)))
        level = level * jnp.repeat(draws, dims[position] // parts).reshape([-1 if axis == position else 1 for axis in range(len(dims))])
    return level


def scatter_about(rng, shape, deviation, bound, cuts=(), kind=jnp.bfloat16):
    level = block_scale(rng, shape, cuts, -0.22, 0.18) if cuts else 1.0
    drawn = jax.random.normal(rng, shape, jnp.float32) * deviation * level
    return jnp.minimum(jnp.maximum(drawn, -bound), bound).astype(kind)


def bell_draw_with(key, shape, width, most, cuts, heavy, kind=jnp.bfloat16):
    result = width * jax.random.normal(key, shape, jnp.float32)
    if cuts:
        result = result * block_scale(key, shape, cuts, -0.22, 0.18)
    return jnp.clip(strengthened(result, jax.random.fold_in(key, 3), *heavy), -most, most).astype(kind)


def setup_inputs(seed: int = 0) -> dict:
    key_of = jax.random.split(jax.random.key(seed), 11)
    inputs = scatter_about(key_of[0], (TOKENS, D), 1.0, 6.0, ((0, 16), (1, 8)))
    cotangent = bell_draw_with(key_of[1], (TOKENS, D), 1.0, 6.0, ((0, 16), (1, 8)), (0, 1, 16, 2.0))
    pre_norm = draw_pre_norm(jax.random.fold_in(key_of[10], 71), 0)
    gate_pre = scatter_about(key_of[3], (TOKENS, FF), 1.5, 8.0, ((0, 16), (1, 8)))
    value_pre = scatter_about(key_of[4], (TOKENS, FF), 1.0, 6.0, ((0, 16), (1, 8)))
    gate_weight = scatter_about(key_of[5], (D, FF), D ** -0.5, 0.109375, ((0, 16), (1, 8)))
    value_weight = scatter_about(key_of[6], (D, FF), D ** -0.5, 0.109375, ((0, 16), (1, 8)))
    down_weight = scatter_about(key_of[7], (FF, D), FF ** -0.5, 0.078125, ((0, 8), (1, 16)))
    conv_taps = scatter_about(key_of[8], (3, FF), 3 ** -0.5, 3.5, ((1, 8),), jnp.float32)
    norm_gain = jnp.clip(1.0 + 0.18 * jax.random.normal(key_of[9], (D,), jnp.float32), 0.1, 1.9)
    return {"inputs": inputs, "cotangent": cotangent, "pre_norm": pre_norm, "gate_pre": gate_pre, "value_pre": value_pre, "gate_weight": gate_weight, "value_weight": value_weight, "down_weight": down_weight, "conv_taps": conv_taps, "norm_gain": norm_gain}


EPSILON = 1e-06

def shifted(values, forward):
    positions = jnp.arange(values.shape[0]) % SEQ
    zeros_row = jnp.zeros((1, values.shape[1]), values.dtype)
    if forward:
        moved = jnp.concatenate([zeros_row, values[:-1]], axis=0)
        keep = positions != 0
    else:
        moved = jnp.concatenate([values[1:], zeros_row], axis=0)
        keep = positions != SEQ - 1
    return jnp.where(keep[:, None], moved, jnp.zeros_like(moved))

def contract_rows(left, right):
    return lax.dot_general(left, right, (((0,), (0,)), ((), ())), preferred_element_type=jnp.float32)

def reference(inputs, cotangent, pre_norm, gate_pre, value_pre, gate_weight, value_weight, down_weight, conv_taps, norm_gain):
    normed = pre_norm.astype(jnp.float32)
    cot_float = cotangent.astype(jnp.float32)
    scaled = norm_gain[None, :] * cot_float
    inverse = lax.rsqrt(lax.optimization_barrier(jnp.sum(normed * normed, axis=1)) / D + EPSILON)
    cross = lax.optimization_barrier(jnp.sum(normed * scaled, axis=1)) / D
    grad_pre = (inverse[:, None] * (scaled - normed * (inverse * inverse * cross)[:, None])).astype(jnp.bfloat16)
    grad_gain = lax.optimization_barrier(jnp.sum(cot_float * normed * inverse[:, None], axis=0))
    gate_float = gate_pre.astype(jnp.float32)
    before = shifted(gate_float, True)
    after = shifted(gate_float, False)
    mixed = conv_taps[0][None] * before + conv_taps[1][None] * gate_float + conv_taps[2][None] * after
    sig = jax.nn.sigmoid(mixed)
    active = mixed * sig
    value_float = value_pre.astype(jnp.float32)
    hidden = (active * value_float).astype(jnp.bfloat16)
    grad_act = lax.dot_general(grad_pre, down_weight, (((1,), (1,)), ((), ())), preferred_element_type=jnp.float32)
    grad_val = (grad_act * active).astype(jnp.bfloat16)
    grad_mixed = grad_act * value_float * sig * (1.0 + mixed * (1.0 - sig))
    grad_taps = jnp.stack([lax.optimization_barrier(jnp.sum(grad_mixed * before, axis=0)), lax.optimization_barrier(jnp.sum(grad_mixed * gate_float, axis=0)), lax.optimization_barrier(jnp.sum(grad_mixed * after, axis=0))], axis=0)
    grad_gpre = (conv_taps[1][None] * grad_mixed + conv_taps[0][None] * shifted(grad_mixed, False) + conv_taps[2][None] * shifted(grad_mixed, True)).astype(jnp.bfloat16)
    block_size = FF // N_TP
    accum = jnp.zeros((inputs.shape[0], D), jnp.float32)
    for block in range(N_TP):
        lower = block * block_size
        upper = lower + block_size
        partial_sum = lax.dot_general(grad_gpre[:, lower:upper], gate_weight[:, lower:upper], (((1,), (1,)), ((), ())), preferred_element_type=jnp.float32)
        partial_sum = partial_sum + lax.dot_general(grad_val[:, lower:upper], value_weight[:, lower:upper], (((1,), (1,)), ((), ())), preferred_element_type=jnp.float32)
        rounded = lax.optimization_barrier(partial_sum.astype(jnp.bfloat16))
        accum = accum + rounded.astype(jnp.float32)
    grad_input = accum.astype(jnp.bfloat16)
    grad_gate = contract_rows(inputs, grad_gpre)
    grad_value = contract_rows(inputs, grad_val)
    grad_down = contract_rows(hidden, grad_pre)
    return (grad_input, grad_gate, grad_value, grad_down, grad_taps, grad_gain)
```

```python
import jax
import jax.numpy as jnp
from jax import lax
from jax.experimental import pallas as pl
from jax.experimental.pallas import tpu as pltpu
from jax.sharding import Mesh
from jax.sharding import PartitionSpec as P

D = 3072
SEQ = 128
EPSILON = 1e-06
HALF = 384
ROWS = 192
TOK = 512
FEAT = 384
BF = jnp.bfloat16
F32 = jnp.float32
MESH = pl.DeviceIdType.MESH


def _mo(v, m):
    return pl.multiple_of(v, m)


class Sems:
    def __init__(self, send, recv):
        self.send, self.recv, self.n, self.all = send, recv, 0, []

    def msg(self, src, dst, **dev):
        i = self.n
        self.n += 1
        m = pltpu.make_async_remote_copy(
            src_ref=src,
            dst_ref=dst,
            send_sem=self.send.at[i],
            recv_sem=self.recv.at[i],
            device_id=dev,
            device_id_type=MESH,
        )
        self.all.append(m)
        return m

    def drain(self):
        for m in self.all:
            m.wait_send()


class Bcast:
    def __init__(self, sems, axis, me, own, slot):
        up, down = lax.rem(me + 1, 4), lax.rem(me + 3, 4)
        to_up, to_down = {axis: up}, {axis: down}
        self.m0 = sems.msg(own(0), slot(me, 0), **to_up)
        self.m1 = sems.msg(own(1), slot(me, 1), **to_down)
        self.m2 = sems.msg(own(1), slot(me, 1), **to_up)
        self.m3 = sems.msg(own(0), slot(me, 0), **to_down)
        self.m4 = sems.msg(slot(down, 0), slot(down, 0), **to_up)
        self.m5 = sems.msg(slot(up, 1), slot(up, 1), **to_down)

    def first(self):
        self.m0.start()
        self.m1.start()

    def second(self):
        self.m2.start()
        self.m3.start()

    def forward(self):
        self.m0.wait_recv()
        self.m4.start()
        self.m1.wait_recv()
        self.m5.start()

    def near(self):
        self.m2.wait_recv()
        self.m3.wait_recv()

    def far(self):
        self.m4.wait_recv()
        self.m5.wait_recv()


def _where():
    z, y = lax.axis_index("z"), lax.axis_index("y")
    x, c = lax.axis_index("x"), lax.axis_index("c")
    yp = y + 1 - 2 * lax.rem(y, 2)
    yh = 3 - y
    yq = yh + 1 - 2 * lax.rem(yh, 2)
    return z, y, x, c, yp, yh, yq


def gather_kernel(
    pre, cot, gain, xin, wdm, wdt, wgm, wgt, pm, pt,
    GP, X, Wd, Wg, PRE, gl,
    st, gpo, ss, rs,
):
    z, y, x, c, yp, yh, yq = _where()
    tp = x * 2 + c
    sems = Sems(ss, rs)

    pf = pre[...].astype(F32)
    cf = cot[...].astype(F32)
    scaled = gain[...] * cf

    def lane_sums(v):
        v = v[:, :128] + v[:, 128:256] + v[:, 256:384]
        return jnp.sum(v.T, axis=0, keepdims=True)

    st[0, 0:1, :] = lane_sums(pf * pf)
    st[0, 1:2, :] = lane_sums(pf * scaled)

    barrier = pltpu.get_barrier_semaphore()
    peers = [{"z": lax.rem(z + 1, 4)}, {"z": lax.rem(z + 3, 4)}, {"y": yp}, {"y": yh}]
    tps = []
    for k in range(1, 8):
        t = lax.rem(tp + k, 8)
        tps.append({"x": t // 2, "c": lax.rem(t, 2)})
    for dev in peers + tps:
        pl.semaphore_signal(barrier, inc=1, device_id=dev, device_id_type=MESH)
    pl.semaphore_wait(barrier, 11)

    stats = [sems.msg(st.at[0], st.at[k], **tps[k - 1]) for k in range(1, 8)]
    for m in stats:
        m.start()

    class Weights:
        def __init__(self, mine, theirs, buf):
            def rows(zz, yy, h=None):
                if h is None:
                    return buf.at[pl.ds(_mo((zz * 4 + yy) * ROWS, 16), ROWS)]
                return buf.at[pl.ds(_mo((zz * 4 + yy) * ROWS + h * 96, 16), 96)]

            self.b0 = Bcast(
                sems, "z", z, lambda h: mine.at[pl.ds(h * 96, 96)], lambda zz, h: rows(zz, y, h)
            )
            self.lo = sems.msg(theirs, rows(z, y), y=yp)
            zs = [z, lax.rem(z + 3, 4), lax.rem(z + 1, 4), lax.rem(z + 2, 4)]
            self.u = [sems.msg(mine if k == 0 else rows(zz, y), rows(zz, y), y=yh) for k, zz in enumerate(zs)]
            self.u4 = sems.msg(rows(z, yp), rows(z, yp), y=yh)
            self.b1 = Bcast(sems, "z", z, lambda h: rows(z, yp, h), lambda zz, h: rows(zz, yp, h))
            self.b2 = Bcast(sems, "z", z, lambda h: rows(z, yq, h), lambda zz, h: rows(zz, yq, h))
            self.keep = lambda: self.store(mine, buf)

        def store(self, mine, buf):
            buf[pl.ds(_mo((z * 4 + y) * ROWS, 16), ROWS), :] = mine[...]

    class Acts:
        def __init__(self, own, buf, kind):
            def slot(xx, h=None):
                lanes = pl.ds(_mo((xx * 2 + c) * FEAT, 128), FEAT)
                if h is None:
                    return buf.at[pl.ds(kind * TOK, TOK), lanes]
                return buf.at[pl.ds(kind * TOK + h * 256, 256), lanes]

            half = (lambda h: own.at[pl.ds(h * 256, 256)]) if kind == 0 else (lambda h: slot(x, h))
            self.b = Bcast(sems, "x", x, half, slot)
            xs = [x, lax.rem(x + 3, 4), lax.rem(x + 1, 4), lax.rem(x + 2, 4)]
            sib = 1 - c
            self.d = [
                sems.msg(own if (k == 0 and kind == 0) else slot(xx), slot(xx), c=sib)
                for k, xx in enumerate(xs)
            ]
            if kind == 0:
                lanes = pl.ds(_mo(tp * FEAT, 128), FEAT)
                self.lo = sems.msg(own, buf.at[pl.ds(TOK, TOK), lanes], y=yp)

        def near(self):
            self.b.near()
            self.d[1].start()
            self.d[2].start()

        def far(self):
            self.b.far()
            self.d[3].start()

        def arrived(self):
            for m in self.d:
                m.wait_recv()

    wd = Weights(wdm, wdt, Wd)
    wg = Weights(wgm, wgt, Wg)
    go, gp = Acts(gpo, GP, 0), Acts(None, GP, 1)
    xo, xp = Acts(xin, X, 0), Acts(None, X, 1)
    plo = sems.msg(pt, PRE.at[pl.ds(TOK, TOK)], y=yp)

    wd.b0.first()
    wd.u[0].start()
    wd.lo.start()
    xo.b.first()
    wd.b0.second()
    xo.d[0].start()

    wd.keep()
    wg.keep()
    PRE[0:TOK, :] = pm[...]
    own_lanes = pl.ds(_mo(tp * FEAT, 128), FEAT)
    X[0:TOK, own_lanes] = xin[...]

    for m in stats:
        m.wait_recv()
    tot = st[0]
    for k in range(1, 8):
        tot = tot + st[k]
    inverse = lax.rsqrt(tot[0:1] / D + EPSILON)
    coef = inverse * inverse * (tot[1:2] / D)

    def column(v):
        v = jnp.broadcast_to(v, (128, TOK)).T
        return jnp.concatenate([v, v, v], axis=1)

    inv = column(inverse)
    pf = pre[...].astype(F32)
    cf = cot[...].astype(F32)
    scaled = gain[...] * cf
    g = (inv * (scaled - pf * column(coef))).astype(BF)
    gpo[...] = g
    GP[0:TOK, own_lanes] = g
    gl[...] = jnp.broadcast_to(jnp.sum(cf * pf * inv, axis=0, keepdims=True), (8, FEAT))

    wd.b0.forward()
    go.b.first()
    go.lo.start()
    go.b.second()
    go.d[0].start()
    wg.lo.start()
    plo.start()
    xo.lo.start()
    wd.b0.near()
    wd.u[1].start()
    wd.u[2].start()
    wd.lo.wait_recv()
    wd.u4.start()
    wd.b1.first()
    wd.b1.second()
    wd.b0.far()
    wd.u[3].start()
    wd.u4.wait_recv()
    wd.b2.first()
    wd.b2.second()
    wd.b1.forward()
    wg.b0.first()
    wg.b0.second()
    wg.u[0].start()
    go.b.forward()
    wd.b2.forward()
    go.lo.wait_recv()
    gp.b.first()
    gp.b.second()
    gp.d[0].start()
    go.near()
    xo.b.second()
    wg.b0.forward()
    wg.b0.near()
    wg.u[1].start()
    wg.u[2].start()
    go.far()
    wg.lo.wait_recv()
    wg.u4.start()
    wg.b1.first()
    wg.b1.second()
    wg.b0.far()
    wg.u[3].start()
    gp.b.forward()
    xo.b.forward()
    gp.near()
    wg.b1.forward()
    wg.u4.wait_recv()
    wg.b2.first()
    wg.b2.second()
    gp.far()
    xo.near()
    wg.b2.forward()
    xo.lo.wait_recv()
    xp.b.first()
    xp.b.second()
    xp.d[0].start()
    xo.far()
    xp.b.forward()
    xp.near()
    xp.far()
    plo.wait_recv()
    for w in (wd, wg):
        w.b1.near()
        w.b1.far()
        w.b2.near()
        w.b2.far()
        for m in w.u:
            m.wait_recv()
    for a in (go, gp, xo, xp):
        a.arrived()
    sems.drain()


N1 = 7 + 2 * 24 + 4 * 10 + 2 + 1


class Scatter:
    def __init__(self, sems, axis, me, chunk, got, sent, rows):
        up, down = lax.rem(me + 1, 4), lax.rem(me + 3, 4)
        far = lax.rem(me + 2, 4)
        to_up, to_down = {axis: up}, {axis: down}
        self.me, self.up, self.down, self.far = me, up, down, far
        self.chunk, self.got, self.sent, self.rows = chunk, got, sent, rows
        self.m0 = sems.msg(chunk(far, 0), got.at[0], **to_up)
        self.m1 = sems.msg(chunk(far, 1), got.at[1], **to_down)
        self.m2 = sems.msg(chunk(up, 1), got.at[2], **to_up)
        self.m3 = sems.msg(chunk(down, 0), got.at[3], **to_down)
        self.m4 = sems.msg(sent.at[0], got.at[4], **to_up)
        self.m5 = sems.msg(sent.at[1], got.at[5], **to_down)

    def raw(self):
        self.m0.start()
        self.m1.start()
        self.m2.start()
        self.m3.start()

    def _add(self, dst, a, b):
        @pl.loop(0, self.rows // 48 if self.rows == 96 else self.rows // 64)
        def _(i):
            n = 48 if self.rows == 96 else 64
            r = pl.ds(_mo(i * n, 16), n)
            dst[r, :] = (a[r, :].astype(F32) + b[r, :].astype(F32)).astype(BF)

    def merge(self):
        self.m0.wait_recv()
        self._add(self.sent.at[0], self.chunk(self.up, 0), self.got.at[0])
        self.m4.start()
        self.m1.wait_recv()
        self._add(self.sent.at[1], self.chunk(self.down, 1), self.got.at[1])
        self.m5.start()

    def last(self, put):
        self.m2.wait_recv()
        self.m3.wait_recv()
        self.m4.wait_recv()
        self.m5.wait_recv()
        n = 48 if self.rows == 96 else 64
        for h, (a, b) in enumerate(((3, 4), (2, 5))):
            own = self.chunk(self.me, h)

            @pl.loop(0, self.rows // n)
            def _(i):
                r = pl.ds(_mo(i * n, 16), n)
                total = own[r, :].astype(F32) + self.got[a, r, :].astype(F32) + self.got[b, r, :].astype(F32)
                put(h, i * n, n, total)


def scatter_kernel(
    Dd, Dg, C, small,
    gi, outd, outg, sums,
    E, MC, xgot, xsent, xout, xin,
    dgot, dsent, dmo, dh, dq, dhq, dl, dlin,
    ggot, gsent, gmo, gh, gq, ghq, gl, glin,
    sz, sy, ss, rs,
):
    z, y, x, c, yp, yh, yq = _where()
    hs = lax.rem((y + 1) // 2, 2)
    sems = Sems(ss, rs)
    barrier = pltpu.get_barrier_semaphore()
    zk = [lax.rem(z + k, 4) for k in range(4)]
    peers = [{"z": zk[1]}, {"z": zk[2]}, {"z": zk[3]}, {"y": yp}, {"y": yh}, {"y": yq}]
    peers += [{"x": lax.rem(x + 1, 4)}, {"x": lax.rem(x + 3, 4)}, {"c": 1 - c}]
    for dev in peers:
        pl.semaphore_signal(barrier, inc=1, device_id=dev, device_id_type=MESH)
    pl.semaphore_wait(barrier, 9)

    class Weights:
        def __init__(self, src, got, sent, mo, hb, q, hq, lo, lin):
            def rows(zz, yy, h=None):
                if h is None:
                    return src.at[pl.ds(_mo((zz * 4 + yy) * ROWS, 16), ROWS)]
                return src.at[pl.ds(_mo((zz * 4 + yy) * ROWS + h * 96, 16), 96)]

            self.rows, self.mo, self.hb, self.q, self.hq, self.lo, self.lin = rows, mo, hb, q, hq, lo, lin
            self.zq = Scatter(sems, "z", z, lambda zz, h: rows(zz, yq, h), got.at[0], sent.at[0], 96)
            self.zp = Scatter(sems, "z", z, lambda zz, h: rows(zz, yp, h), got.at[1], sent.at[1], 96)
            self.zo = Scatter(sems, "z", z, lambda zz, h: mo.at[zz, pl.ds(h * 96, 96)], got.at[2], sent.at[2], 96)
            self.v = [sems.msg(rows(zk[k], yh), hb.at[k], y=yh) for k in range(4)]
            self.v4 = sems.msg(q, hq, y=yh)
            self.l = sems.msg(lo, lin, y=yp)

        def start(self):
            self.zq.raw()
            for k in (2, 1, 3, 0):
                self.v[k].start()

        def merge_hi(self):
            for k in (2, 1, 3, 0):
                self.v[k].wait_recv()
                own = self.rows(zk[k], y)

                @pl.loop(0, 4)
                def _(i):
                    r = pl.ds(_mo(i * 48, 16), 48)
                    self.mo[zk[k], r, :] = (own[r, :].astype(F32) + self.hb[k, r, :].astype(F32)).astype(BF)

        def q_out(self):
            def put(h, i, n, total):
                self.q[pl.ds(_mo(h * 96 + i, 16), n), :] = total.astype(BF)

            self.zq.last(put)
            self.v4.start()

        def p_out(self):
            self.v4.wait_recv()

            def put(h, i, n, total):
                r = pl.ds(_mo(h * 96 + i, 16), n)
                self.lo[r, :] = (total + self.hq[r, :].astype(F32)).astype(BF)

            self.zp.last(put)
            self.l.start()

        def o_out(self, out):
            def put(h, i, n, total):
                out[hs, pl.ds(_mo(h * 96 + i, 16), n), :] = total

            self.zo.last(put)

        def final(self, out):
            self.l.wait_recv()

            @pl.loop(0, 4)
            def _(i):
                r = pl.ds(_mo(i * 48, 16), 48)
                out[1 - hs, r, :] = self.lin[r, :].astype(F32)

    wd = Weights(Dd, dgot, dsent, dmo, dh, dq, dhq, dl, dlin)
    wg = Weights(Dg, ggot, gsent, gmo, gh, gq, ghq, gl, glin)

    sib = 1 - c

    def lanes(xx, cc):
        return pl.ds(_mo((xx * 2 + cc) * FEAT, 128), FEAT)

    xk = [lax.rem(x + k, 4) for k in range(4)]
    e = [sems.msg(C.at[:, lanes(xk[k], sib)], E.at[k], c=sib) for k in range(4)]
    xs = Scatter(sems, "x", x, lambda xx, h: MC.at[xx, pl.ds(h * TOK, TOK)], xgot, xsent, TOK)
    xl = sems.msg(xout, xin, y=yp)
    sz_m = [sems.msg(small, sz.at[k - 1], z=zk[k]) for k in (1, 2, 3)]
    sy_m = [sems.msg(sy.at[3], sy.at[k], y=yy) for k, yy in enumerate((yh, yp, yq))]

    for k in (2, 1, 3, 0):
        e[k].start()
    for m in sz_m:
        m.start()
    wd.start()
    wg.start()
    wd.zp.raw()
    wg.zp.raw()
    for k in (2, 1, 3, 0):
        e[k].wait_recv()

        @pl.loop(0, 16)
        def _(i):
            r = pl.ds(_mo(i * 64, 16), 64)
            MC[xk[k], r, :] = (C[r, lanes(xk[k], c)].astype(F32) + E[k, r, :].astype(F32)).astype(BF)

    xs.raw()
    for m in sz_m:
        m.wait_recv()
    sy[3] = small[...] + sz[0] + sz[1] + sz[2]
    wd.merge_hi()
    wd.zo.raw()
    for m in sy_m:
        m.start()
    wd.zq.merge()
    wd.q_out()
    xs.merge()
    wg.merge_hi()
    wg.zo.raw()
    wg.zq.merge()
    wd.zp.merge()
    wd.p_out()
    wg.zp.merge()
    wd.zo.merge()
    wg.q_out()
    wg.zo.merge()

    def put(h, i, n, total):
        r = pl.ds(_mo(i, 16), n)
        if h == 0:
            gi32[r, :] = total
        else:
            xout[r, :] = total.astype(BF)

    gi32 = MC.at[0]

    def put_bf(h, i, n, total):
        r = pl.ds(_mo(i, 16), n)
        if h == 0:
            gi[r, :] = total.astype(BF)
        else:
            xout[r, :] = total.astype(BF)

    xs.last(put_bf)
    xl.start()
    wd.o_out(outd)
    for m in sy_m:
        m.wait_recv()
    sums[hs] = sy[3] + sy[0]
    sums[1 - hs] = sy[1] + sy[2]
    wd.final(outd)
    wg.p_out()
    xl.wait_recv()

    @pl.loop(0, 8)
    def _(i):
        r = pl.ds(_mo(i * 64, 16), 64)
        gi[r, :] = (gi[r, :].astype(F32) + xin[r, :].astype(F32)).astype(BF)

    wg.o_out(outg)
    wg.final(outg)
    sems.drain()


N2 = 2 * 24 + 4 + 6 + 1 + 6


def shifted(values, forward):
    positions = jnp.arange(values.shape[0]) % SEQ
    zeros_row = jnp.zeros((1, values.shape[1]), values.dtype)
    if forward:
        moved = jnp.concatenate([zeros_row, values[:-1]], axis=0)
        keep = positions != 0
    else:
        moved = jnp.concatenate([values[1:], zeros_row], axis=0)
        keep = positions != SEQ - 1
    return jnp.where(keep[:, None], moved, jnp.zeros_like(moved))


def dot(left, right, dims):
    return lax.dot_general(left, right, ((dims[0], dims[1]), ((), ())), preferred_element_type=F32)


VM = pl.BlockSpec(memory_space=pltpu.VMEM)


def on_device(
    inputs, cotangent, pre_norm, gate_pre, value_pre, gate_weight, value_weight, down_weight, conv_taps, norm_gain
):
    y = lax.axis_index("y")
    hs = ((y + 1) // 2) % 2

    def halves(w):
        w = jnp.pad(w, ((0, 0), (0, 2 * HALF - w.shape[1])))
        a, b = w[:, :HALF], w[:, HALF:]
        return jnp.where(hs == 0, a, b), jnp.where(hs == 0, b, a)

    wdm, wdt = halves(down_weight.T)
    gm, gt = halves(gate_weight)
    vm, vt = halves(value_weight)
    pgm, pgt = halves(gate_pre)
    pvm, pvt = halves(value_pre)
    taps, _ = halves(conv_taps)
    cat = lambda a, b: jnp.concatenate([a, b], axis=1)
    GP, X, Wd, Wg, PRE, gl = pl.pallas_call(
        gather_kernel,
        out_shape=(
            jax.ShapeDtypeStruct((2 * TOK, D), BF),
            jax.ShapeDtypeStruct((2 * TOK, D), BF),
            jax.ShapeDtypeStruct((D, HALF), BF),
            jax.ShapeDtypeStruct((D, 2 * HALF), BF),
            jax.ShapeDtypeStruct((2 * TOK, 2 * HALF), BF),
            jax.ShapeDtypeStruct((8, FEAT), F32),
        ),
        in_specs=[VM] * 10,
        out_specs=(VM,) * 6,
        scratch_shapes=[
            pltpu.VMEM((8, 8, TOK), F32),
            pltpu.VMEM((TOK, FEAT), BF),
            pltpu.SemaphoreType.DMA((N1,)),
            pltpu.SemaphoreType.DMA((N1,)),
        ],
        compiler_params=pltpu.CompilerParams(
            collective_id=0, has_side_effects=True, vmem_limit_bytes=60 * 1024 * 1024
        ),
        name="gather",
    )(
        pre_norm, cotangent, norm_gain[None, :], inputs, wdm, wdt, cat(gm, vm), cat(gt, vt), cat(pgm, pvm), cat(pgt, pvt)
    )

    grad_act = dot(GP, Wd, ((1,), (0,)))
    gate_float = PRE[:, :HALF].astype(F32)
    value_float = PRE[:, HALF:].astype(F32)
    before = shifted(gate_float, True)
    after = shifted(gate_float, False)
    mixed = taps[0][None] * before + taps[1][None] * gate_float + taps[2][None] * after
    sig = jax.nn.sigmoid(mixed)
    active = mixed * sig
    hidden = (active * value_float).astype(BF)
    grad_val = (grad_act * active).astype(BF)
    grad_mixed = grad_act * value_float * sig * (1.0 + mixed * (1.0 - sig))
    taps_local = [jnp.sum(grad_mixed * v, axis=0, keepdims=True) for v in (before, gate_float, after)]
    grad_gpre = (
        taps[1][None] * grad_mixed
        + taps[0][None] * shifted(grad_mixed, False)
        + taps[2][None] * shifted(grad_mixed, True)
    ).astype(BF)
    G = cat(grad_gpre, grad_val)
    contrib = dot(G, Wg, ((1,), (1,))).astype(BF)
    Dd = dot(GP, hidden, ((0,), (0,))).astype(BF)
    Dg = dot(X, G, ((0,), (0,))).astype(BF)
    small = jnp.concatenate(taps_local + [gl[:5]], axis=0)

    def wscratch(n):
        return [
            pltpu.VMEM((3, 6, 96, n), BF),
            pltpu.VMEM((3, 2, 96, n), BF),
            pltpu.VMEM((4, ROWS, n), BF),
            pltpu.VMEM((4, ROWS, n), BF),
            pltpu.VMEM((ROWS, n), BF),
            pltpu.VMEM((ROWS, n), BF),
            pltpu.VMEM((ROWS, n), BF),
            pltpu.VMEM((ROWS, n), BF),
        ]

    gi, outd, outg, sums = pl.pallas_call(
        scatter_kernel,
        out_shape=(
            jax.ShapeDtypeStruct((TOK, FEAT), BF),
            jax.ShapeDtypeStruct((2, ROWS, HALF), F32),
            jax.ShapeDtypeStruct((2, ROWS, 2 * HALF), F32),
            jax.ShapeDtypeStruct((2, 8, FEAT), F32),
        ),
        in_specs=[VM] * 4,
        out_specs=(VM,) * 4,
        scratch_shapes=[
            pltpu.VMEM((4, 2 * TOK, FEAT), BF),
            pltpu.VMEM((4, 2 * TOK, FEAT), BF),
            pltpu.VMEM((6, TOK, FEAT), BF),
            pltpu.VMEM((2, TOK, FEAT), BF),
            pltpu.VMEM((TOK, FEAT), BF),
            pltpu.VMEM((TOK, FEAT), BF),
        ]
        + wscratch(HALF)
        + wscratch(2 * HALF)
        + [
            pltpu.VMEM((3, 8, FEAT), F32),
            pltpu.VMEM((4, 8, FEAT), F32),
            pltpu.SemaphoreType.DMA((N2,)),
            pltpu.SemaphoreType.DMA((N2,)),
        ],
        compiler_params=pltpu.CompilerParams(
            collective_id=1, has_side_effects=True, vmem_limit_bytes=60 * 1024 * 1024
        ),
        name="scatter",
    )(Dd, Dg, contrib, small)

    rest = gate_pre.shape[1] - HALF
    joined = lambda a, b: jnp.concatenate([a, b[:, :rest]], axis=1)
    grad_gate = joined(outg[0, :, :HALF], outg[1, :, :HALF])
    grad_value = joined(outg[0, :, HALF:], outg[1, :, HALF:])
    grad_down = joined(outd[0], outd[1]).T
    grad_taps = joined(sums[0, :3], sums[1, :3])
    grad_gain = sums[0, 3] + sums[1, 3]
    return (gi, grad_gate, grad_value, grad_down, grad_taps, grad_gain)


def solution(mesh):
    split = Mesh(mesh.devices.reshape(4, 4, 4, 2), ("z", "y", "x", "c"))
    fs, tp = ("z", "y"), ("x", "c")
    both, across = P(fs, tp), P(tp, fs)
    in_specs = (both, both, both, both, both, both, both, across, P(None, tp), P(tp))
    out_specs = (both, both, both, across, P(None, tp), P(tp))
    return jax.shard_map(on_device, mesh=split, in_specs=in_specs, out_specs=out_specs, check_vma=False)
```

```python
import jax
import jax.numpy as jnp
from jax import lax
from jax.experimental import pallas as pl
from jax.experimental.pallas import tpu as pltpu
from jax.sharding import Mesh
from jax.sharding import PartitionSpec as P

D = 3072
SEQ = 128
EPSILON = 1e-06
HALF = 384
ROWS = 192
TOK = 512
FEAT = 384
BF = jnp.bfloat16
F32 = jnp.float32
MESH = pl.DeviceIdType.MESH


def _mo(v, m):
    return pl.multiple_of(v, m)


class Sems:
    def __init__(self, send, recv):
        self.send, self.recv, self.n, self.all = send, recv, 0, []

    def msg(self, src, dst, **dev):
        i = self.n
        self.n += 1
        m = pltpu.make_async_remote_copy(
            src_ref=src,
            dst_ref=dst,
            send_sem=self.send.at[i],
            recv_sem=self.recv.at[i],
            device_id=dev,
            device_id_type=MESH,
        )
        self.all.append(m)
        return m

    def drain(self):
        for m in self.all:
            m.wait_send()


class Bcast:
    def __init__(self, sems, axis, me, own, slot):
        up, down = lax.rem(me + 1, 4), lax.rem(me + 3, 4)
        to_up, to_down = {axis: up}, {axis: down}
        self.m0 = sems.msg(own(0), slot(me, 0), **to_up)
        self.m1 = sems.msg(own(1), slot(me, 1), **to_down)
        self.m2 = sems.msg(own(1), slot(me, 1), **to_up)
        self.m3 = sems.msg(own(0), slot(me, 0), **to_down)
        self.m4 = sems.msg(slot(down, 0), slot(down, 0), **to_up)
        self.m5 = sems.msg(slot(up, 1), slot(up, 1), **to_down)

    def first(self):
        self.m0.start()
        self.m1.start()

    def second(self):
        self.m2.start()
        self.m3.start()

    def forward(self):
        self.m0.wait_recv()
        self.m4.start()
        self.m1.wait_recv()
        self.m5.start()

    def near(self):
        self.m2.wait_recv()
        self.m3.wait_recv()

    def far(self):
        self.m4.wait_recv()
        self.m5.wait_recv()


class Scatter:
    def __init__(self, sems, axis, me, chunk, got, rows, step):
        up, down = lax.rem(me + 1, 4), lax.rem(me + 3, 4)
        far = lax.rem(me + 2, 4)
        to_up, to_down = {axis: up}, {axis: down}
        self.me, self.up, self.down = me, up, down
        self.chunk, self.got, self.rows, self.step = chunk, got, rows, step
        self.m0 = sems.msg(chunk(far, 0), got.at[0], **to_up)
        self.m1 = sems.msg(chunk(far, 1), got.at[1], **to_down)
        self.m2 = sems.msg(chunk(up, 1), got.at[2], **to_up)
        self.m3 = sems.msg(chunk(down, 0), got.at[3], **to_down)
        self.m4 = sems.msg(chunk(up, 0), got.at[4], **to_up)
        self.m5 = sems.msg(chunk(down, 1), got.at[5], **to_down)

    def far(self):
        self.m0.start()
        self.m1.start()

    def near(self):
        self.m2.start()
        self.m3.start()

    def raw(self):
        self.far()
        self.near()

    def merge(self):
        self.m0.wait_recv()
        add_to(self.chunk(self.up, 0), self.got.at[0], self.rows, self.step)
        self.m4.start()
        self.m1.wait_recv()
        add_to(self.chunk(self.down, 1), self.got.at[1], self.rows, self.step)
        self.m5.start()

    def last(self, put):
        self.m2.wait_recv()
        self.m3.wait_recv()
        self.m4.wait_recv()
        self.m5.wait_recv()
        n = self.step
        for h, (a, b) in enumerate(((3, 4), (2, 5))):
            own = self.chunk(self.me, h)

            @pl.loop(0, self.rows // n)
            def _(i):
                r = pl.ds(_mo(i * n, 16), n)
                put(h, i * n, n, own[r, :].astype(F32) + self.got[a, r, :].astype(F32) + self.got[b, r, :].astype(F32))


def add_to(dst, src, rows, step):
    @pl.loop(0, rows // step)
    def _(i):
        r = pl.ds(_mo(i * step, 16), step)
        dst[r, :] = (dst[r, :].astype(F32) + src[r, :].astype(F32)).astype(BF)


def mm(a, b, ca, cb):
    return lax.dot_general(a, b, (((ca,), (cb,)), ((), ())), preferred_element_type=F32)


def kernel(
    pre, cot, gain, xin, down, gatew, valuew, gatep, valuep, taps,
    gi, gg_out, gv_out, gd_out, gt_out, gn_out,
    GP, X, Wd, Wg, PRE, st, gpo, wdm, wdt, wgm, wgt, pt, tap,
    GA, hid, G, tacc, Dd, Dg, CS, MC, E, xgot, xlin,
    dgot, dhb, dhq, dlin, ggot, ghb, ghq, glin,
    small, sz, sy, ss, rs,
):
    z, y = lax.axis_index("z"), lax.axis_index("y")
    x, c = lax.axis_index("x"), lax.axis_index("c")
    yp = y + 1 - 2 * lax.rem(y, 2)
    yh = 3 - y
    yq = yh + 1 - 2 * lax.rem(yh, 2)
    hs = lax.rem((y + 1) // 2, 2)
    sib = 1 - c
    tp = x * 2 + c
    zk = [lax.rem(z + k, 4) for k in range(4)]
    xk = [lax.rem(x + k, 4) for k in range(4)]
    sems = Sems(ss, rs)

    barrier = pltpu.get_barrier_semaphore()
    peers = [{"z": zk[1]}, {"z": zk[2]}, {"z": zk[3]}, {"y": yp}, {"y": yh}, {"y": yq}]
    tps = []
    for k in range(1, 8):
        t = lax.rem(tp + k, 8)
        tps.append({"x": t // 2, "c": lax.rem(t, 2)})
    for dev in peers + tps:
        pl.semaphore_signal(barrier, inc=1, device_id=dev, device_id_type=MESH)

    def lane_sums(v):
        v = v[:, :128] + v[:, 128:256] + v[:, 256:384]
        return jnp.sum(v.T, axis=0, keepdims=True)

    pf = pre[...].astype(F32)
    cf = cot[...].astype(F32)
    scaled = gain[...] * cf
    st[0, 0:1, :] = lane_sums(pf * pf)
    st[0, 1:2, :] = lane_sums(pf * scaled)

    def split(src, mine, theirs):
        n = src.shape[0]
        rest = src.shape[1] - HALF
        fill = jnp.zeros((n, HALF - rest), src.dtype)

        @pl.when(hs == 0)
        def _():
            mine[...] = src[:, :HALF]
            if theirs is not None:
                theirs[:, :rest] = src[:, HALF:]
                theirs[:, rest:] = fill

        @pl.when(hs == 1)
        def _():
            mine[:, :rest] = src[:, HALF:]
            mine[:, rest:] = fill
            if theirs is not None:
                theirs[...] = src[:, :HALF]

    split(down, wdm, wdt)

    class Gather:
        def __init__(self, mine, theirs, buf):
            def rows(zz, yy, h=None):
                if h is None:
                    return buf.at[pl.ds(_mo((zz * 4 + yy) * ROWS, 16), ROWS)]
                return buf.at[pl.ds(_mo((zz * 4 + yy) * ROWS + h * 96, 16), 96)]

            self.b0 = Bcast(
                sems, "z", z, lambda h: mine.at[pl.ds(h * 96, 96)], lambda zz, h: rows(zz, y, h)
            )
            self.lo = sems.msg(theirs, rows(z, y), y=yp)
            zs = [zk[0], zk[3], zk[1], zk[2]]
            self.u = [sems.msg(mine if k == 0 else rows(zz, y), rows(zz, y), y=yh) for k, zz in enumerate(zs)]
            self.u4 = sems.msg(rows(z, yp), rows(z, yp), y=yh)
            self.b1 = Bcast(sems, "z", z, lambda h: rows(z, yp, h), lambda zz, h: rows(zz, yp, h))
            self.b2 = Bcast(sems, "z", z, lambda h: rows(z, yq, h), lambda zz, h: rows(zz, yq, h))
            self.mine, self.buf = mine, buf

        def keep(self):
            self.buf[pl.ds(_mo((z * 4 + y) * ROWS, 16), ROWS), :] = self.mine[...]

        def near(self):
            self.b0.near()
            self.u[1].start()
            self.u[2].start()

        def far(self):
            self.b0.far()
            self.u[3].start()

        def partner(self):
            self.lo.wait_recv()
            self.u4.start()
            self.b1.first()
            self.b1.second()

        def across(self):
            self.u4.wait_recv()
            self.b2.first()
            self.b2.second()

        def arrived(self):
            self.b1.near()
            self.b1.far()
            self.b2.near()
            self.b2.far()
            for m in self.u:
                m.wait_recv()

    class Acts:
        def __init__(self, own, buf, kind):
            def slot(xx, h=None):
                lanes = pl.ds(_mo((xx * 2 + c) * FEAT, 128), FEAT)
                if h is None:
                    return buf.at[pl.ds(kind * TOK, TOK), lanes]
                return buf.at[pl.ds(kind * TOK + h * 256, 256), lanes]

            half = (lambda h: own.at[pl.ds(h * 256, 256)]) if kind == 0 else (lambda h: slot(x, h))
            self.b = Bcast(sems, "x", x, half, slot)
            xs = [xk[0], xk[3], xk[1], xk[2]]
            self.d = [
                sems.msg(own if (k == 0 and kind == 0) else slot(xx), slot(xx), c=sib)
                for k, xx in enumerate(xs)
            ]
            if kind == 0:
                lanes = pl.ds(_mo(tp * FEAT, 128), FEAT)
                self.lo = sems.msg(own, buf.at[pl.ds(TOK, TOK), lanes], y=yp)

        def near(self):
            self.b.near()
            self.d[1].start()
            self.d[2].start()

        def far(self):
            self.b.far()
            self.d[3].start()

        def arrived(self):
            for m in self.d:
                m.wait_recv()

    class Reduce:
        def __init__(self, src, got, hb, hq, lin):
            def rows(zz, yy, h=None):
                if h is None:
                    return src.at[pl.ds(_mo((zz * 4 + yy) * ROWS, 16), ROWS)]
                return src.at[pl.ds(_mo((zz * 4 + yy) * ROWS + h * 96, 16), 96)]

            self.rows, self.hb, self.hq, self.lin = rows, hb, hq, lin
            self.zq = Scatter(sems, "z", z, lambda zz, h: rows(zz, yq, h), got.at[0], 96, 48)
            self.zp = Scatter(sems, "z", z, lambda zz, h: rows(zz, yp, h), got.at[1], 96, 48)
            self.zo = Scatter(sems, "z", z, lambda zz, h: rows(zz, y, h), got.at[2], 96, 48)
            self.v = [sems.msg(rows(zk[k], yh), hb.at[k], y=yh) for k in range(4)]
            self.v4 = sems.msg(rows(z, yq), hq, y=yh)
            self.l = sems.msg(rows(z, yp), lin, y=yp)

        def merge_hi(self, ks):
            for k in ks:
                self.v[k].wait_recv()
                add_to(self.rows(zk[k], y), self.hb.at[k], ROWS, 48)

        def q_out(self):
            own = self.rows(z, yq)

            def put(h, i, n, total):
                own[pl.ds(_mo(h * 96 + i, 16), n), :] = total.astype(BF)

            self.zq.last(put)
            self.v4.start()

        def p_out(self):
            self.v4.wait_recv()
            own = self.rows(z, yp)

            def put(h, i, n, total):
                r = pl.ds(_mo(h * 96 + i, 16), n)
                own[r, :] = (total + self.hq[r, :].astype(F32)).astype(BF)

            self.zp.last(put)
            self.l.start()

        def o_out(self, outs):
            def put(h, i, n, total):
                write(outs, hs, h * 96 + i, n, total)

            self.zo.last(put)

        def final(self, outs):
            self.l.wait_recv()

            @pl.loop(0, 4)
            def _(i):
                write(outs, 1 - hs, i * 48, 48, self.lin[pl.ds(_mo(i * 48, 16), 48), :].astype(F32))

    def write(outs, half, row, n, value):
        r = pl.ds(_mo(row, 16), n)
        for j, out in enumerate(outs):
            part = value[:, j * HALF : (j + 1) * HALF]
            rest = out.shape[1] - HALF

            @pl.when(half == 0)
            def _():
                out[r, :HALF] = part

            @pl.when(half == 1)
            def _():
                out[r, HALF:] = part[:, :rest]

    gd = Gather(wdm, wdt, Wd)
    gw = Gather(wgm, wgt, Wg)
    go, gp = Acts(gpo, GP, 0), Acts(None, GP, 1)
    xo, xp = Acts(xin, X, 0), Acts(None, X, 1)
    plo = sems.msg(pt, PRE.at[pl.ds(TOK, TOK)], y=yp)
    stats = [sems.msg(st.at[0], st.at[k], **tps[k - 1]) for k in range(1, 8)]
    sd = Reduce(Dd, dgot, dhb, dhq, dlin)
    sw = Reduce(Dg, ggot, ghb, ghq, glin)
    e = [sems.msg(CS.at[k], E.at[k], c=sib) for k in range(4)]
    xs = Scatter(sems, "x", x, lambda xx, h: MC.at[lax.rem(xx - x + 4, 4), pl.ds(h * TOK, TOK)], xgot, TOK, 64)
    xl = sems.msg(MC.at[0, pl.ds(TOK, TOK)], xlin, y=yp)
    sz_m = [sems.msg(small, sz.at[k - 1], z=zk[k]) for k in (1, 2, 3)]
    sy_m = [sems.msg(sy.at[3], sy.at[k], y=yy) for k, yy in enumerate((yh, yp, yq))]

    def grad_act(kind):
        @pl.loop(0, 2)
        def _(i):
            r = pl.ds(_mo(kind * TOK + i * 256, 256), 256)
            GA[r, :] = mm(GP[r, :], Wd[...], 1, 0)

    def middle(kind, lo, hi):
        row = lax.broadcasted_iota(jnp.int32, (SEQ, 128), 0)

        def prev(v):
            return jnp.where(row == 0, 0.0, pltpu.roll(v, 1, 0))

        def succ(v):
            return jnp.where(row == SEQ - 1, 0.0, pltpu.roll(v, SEQ - 1, 0))

        @pl.loop(lo, hi)
        def _(i):
            r = pl.ds(_mo(kind * TOK + (i // 3) * SEQ, SEQ), SEQ)
            at = lax.rem(i, 3) * 128
            lanes, lanes2 = pl.ds(_mo(at, 128), 128), pl.ds(_mo(HALF + at, 128), 128)
            gate = PRE[r, lanes].astype(F32)
            value = PRE[r, lanes2].astype(F32)
            t0, t1, t2 = (tap[k : k + 1, lanes] for k in range(3))
            before, after = prev(gate), succ(gate)
            mixed = t0 * before + t1 * gate + t2 * after
            sig = jax.nn.sigmoid(mixed)
            active = mixed * sig
            ga = GA[r, lanes]
            hid[r, lanes] = (active * value).astype(BF)
            G[r, lanes2] = (ga * active).astype(BF)
            gm = ga * value * sig * (1.0 + mixed * (1.0 - sig))
            G[r, lanes] = (t1 * gm + t0 * succ(gm) + t2 * prev(gm)).astype(BF)
            for k, v in enumerate((before, gate, after)):
                tacc[k, :, lanes] += jnp.sum((gm * v).reshape(SEQ // 8, 8, 128), axis=0)

    def block(dst, left, right, zz, yy):
        at = _mo((zz * 2 + yy // 2) * FEAT, 128)
        dst[pl.ds(at, FEAT), :] = mm(left[:, pl.ds(at, FEAT)], right[...], 0, 0).astype(BF)

    def blocks(dst, left, right, yy, first):
        @pl.loop(0, 2)
        def _(k):
            zz = lax.rem(z + 2 - k + 4, 4) if first else lax.rem(z + 3 + k, 4)
            block(dst, left, right, zz, yy)

    def contrib(dst, cc, first):
        @pl.loop(0, 2)
        def _(i):
            k = 2 - i if first else lax.rem(3 + i, 4)
            at = _mo((lax.rem(x + k, 4) * 2 + cc) * FEAT, 128)
            dst[k] = mm(G[...], Wg[pl.ds(at, FEAT), :], 1, 1).astype(BF)

    pl.semaphore_wait(barrier, 13)
    for m in stats:
        m.start()
    gd.b0.first()
    gd.u[0].start()
    gd.lo.start()
    xo.b.first()
    gd.b0.second()
    xo.d[0].start()
    split(gatew, wgm.at[:, 0:HALF], wgt.at[:, 0:HALF])
    split(valuew, wgm.at[:, HALF : 2 * HALF], wgt.at[:, HALF : 2 * HALF])
    split(taps, tap, None)
    gd.keep()
    gw.keep()
    own_lanes = pl.ds(_mo(tp * FEAT, 128), FEAT)
    X[0:TOK, own_lanes] = xin[...]
    tacc[...] = jnp.zeros_like(tacc)

    for m in stats:
        m.wait_recv()
    tot = st[0]
    for k in range(1, 8):
        tot = tot + st[k]
    inverse = lax.rsqrt(tot[0:1] / D + EPSILON)
    coef = inverse * inverse * (tot[1:2] / D)

    def column(v):
        v = jnp.broadcast_to(v, (128, TOK)).T
        return jnp.concatenate([v, v, v], axis=1)

    inv = column(inverse)
    pf = pre[...].astype(F32)
    cf = cot[...].astype(F32)
    scaled = gain[...] * cf
    g = (inv * (scaled - pf * column(coef))).astype(BF)
    gpo[...] = g
    GP[0:TOK, own_lanes] = g
    gain_sum = jnp.sum(cf * pf * inv, axis=0, keepdims=True)
    small[...] = jnp.broadcast_to(gain_sum, (8, FEAT))

    gd.b0.forward()
    go.b.first()
    go.lo.start()
    go.b.second()
    go.d[0].start()
    split(gatep, PRE.at[0:TOK, 0:HALF], pt.at[:, 0:HALF])
    split(valuep, PRE.at[0:TOK, HALF : 2 * HALF], pt.at[:, HALF : 2 * HALF])
    gw.lo.start()
    plo.start()
    xo.lo.start()
    gd.near()
    gd.partner()
    gd.far()
    gd.across()
    gd.b1.forward()
    gw.b0.first()
    gw.b0.second()
    gw.u[0].start()
    go.b.forward()
    gd.b2.forward()
    go.lo.wait_recv()
    gp.b.first()
    gp.b.second()
    gp.d[0].start()
    xo.b.second()
    go.near()
    gw.b0.forward()
    gw.near()
    go.far()
    gw.partner()
    gw.far()
    gd.arrived()
    go.arrived()
    grad_act(0)
    gw.b1.forward()
    gp.b.forward()
    gw.across()
    middle(0, 0, 6)
    gp.near()
    xo.b.forward()
    middle(0, 6, 12)
    gw.b2.forward()
    xo.lo.wait_recv()
    xp.b.first()
    xp.b.second()
    xp.d[0].start()
    gp.far()
    plo.wait_recv()
    gp.arrived()
    grad_act(1)
    xo.near()
    xp.b.forward()
    middle(1, 0, 6)
    xo.far()
    middle(1, 6, 12)
    blocks(Dd, GP, hid, yh, True)
    sd.v[2].start()
    sd.zq.far()
    sd.v[1].start()
    blocks(Dd, GP, hid, yh, False)
    sd.zq.near()
    sd.v[3].start()
    sd.v[0].start()
    blocks(Dd, GP, hid, y, True)
    xp.near()
    sd.zp.far()
    blocks(Dd, GP, hid, y, False)
    sd.zp.near()
    for k in range(3):
        small[k : k + 1, :] = jnp.sum(tacc[k], axis=0, keepdims=True)
    for m in sz_m:
        m.start()
    gw.arrived()
    sd.zq.merge()
    xp.far()
    contrib(CS, sib, True)
    e[2].start()
    e[1].start()
    contrib(CS, sib, False)
    e[3].start()
    e[0].start()
    sd.merge_hi((2, 1, 3))
    sd.zo.raw()
    sd.q_out()
    sd.zp.merge()
    xo.arrived()
    xp.arrived()
    blocks(Dg, X, G, yh, True)
    sw.v[2].start()
    sw.zq.far()
    sw.v[1].start()
    blocks(Dg, X, G, yh, False)
    sw.zq.near()
    sw.v[3].start()
    sw.v[0].start()
    sd.zo.merge()
    blocks(Dg, X, G, y, True)
    sw.zp.far()
    blocks(Dg, X, G, y, False)
    sw.zp.near()
    contrib(MC, c, True)
    for k in (2, 1):
        e[k].wait_recv()
        add_to(MC.at[k], E.at[k], 2 * TOK, 64)
    xs.far()
    contrib(MC, c, False)
    for k in (3, 0):
        e[k].wait_recv()
        add_to(MC.at[k], E.at[k], 2 * TOK, 64)
    xs.near()
    sw.merge_hi((2, 1, 3))
    sw.zo.raw()
    sw.zq.merge()
    for m in sz_m:
        m.wait_recv()
    sy[3] = small[...] + sz[0] + sz[1] + sz[2]
    sd.p_out()
    for m in sy_m:
        m.start()
    sw.q_out()
    xs.merge()
    sw.zp.merge()
    sw.zo.merge()
    sd.merge_hi((0,))
    sd.o_out((gd_out,))
    sd.final((gd_out,))
    sw.merge_hi((0,))
    for m in sy_m:
        m.wait_recv()
    rest = gt_out.shape[1] - HALF
    mine_sum = sy[3] + sy[0]
    their_sum = sy[1] + sy[2]

    @pl.when(hs == 0)
    def _():
        gt_out[:, :HALF] = mine_sum[0:3]
        gt_out[:, HALF:] = their_sum[0:3, :rest]

    @pl.when(hs == 1)
    def _():
        gt_out[:, :HALF] = their_sum[0:3]
        gt_out[:, HALF:] = mine_sum[0:3, :rest]

    gn_out[...] = mine_sum[3:4] + their_sum[3:4]

    def put_x(h, i, n, total):
        r = pl.ds(_mo(i, 16), n)
        if h == 0:
            GA[r, :] = total
        else:
            MC[0, pl.ds(_mo(TOK + i, 16), n), :] = total.astype(BF)

    xs.last(put_x)
    xl.start()
    sw.p_out()
    sw.o_out((gg_out, gv_out))
    xl.wait_recv()

    @pl.loop(0, 8)
    def _(i):
        r = pl.ds(_mo(i * 64, 16), 64)
        gi[r, :] = (GA[r, :] + xlin[r, :].astype(F32)).astype(BF)

    sw.final((gg_out, gv_out))
    sems.drain()


N = 7 + 2 * 24 + 4 * 10 + 2 + 1 + 2 * 24 + 4 + 6 + 1 + 6
VM = pl.BlockSpec(memory_space=pltpu.VMEM)


def on_device(
    inputs, cotangent, pre_norm, gate_pre, value_pre, gate_weight, value_weight, down_weight, conv_taps, norm_gain
):
    width = gate_pre.shape[1]

    def vm(*shape, dtype=BF):
        return pltpu.VMEM(shape, dtype)

    def wscratch(n):
        return [vm(3, 6, 96, n), vm(4, ROWS, n), vm(ROWS, n), vm(ROWS, n)]

    two = 2 * TOK
    gi, gg, gv, gd, gt, gn = pl.pallas_call(
        kernel,
        out_shape=(
            jax.ShapeDtypeStruct((TOK, FEAT), BF),
            jax.ShapeDtypeStruct((ROWS, width), F32),
            jax.ShapeDtypeStruct((ROWS, width), F32),
            jax.ShapeDtypeStruct((ROWS, width), F32),
            jax.ShapeDtypeStruct((3, width), F32),
            jax.ShapeDtypeStruct((1, FEAT), F32),
        ),
        in_specs=[VM] * 10,
        out_specs=(VM,) * 6,
        scratch_shapes=[
            vm(two, D), vm(two, D), vm(D, HALF), vm(D, 2 * HALF), vm(two, 2 * HALF),
            vm(8, 8, TOK, dtype=F32), vm(TOK, FEAT),
            vm(ROWS, HALF), vm(ROWS, HALF), vm(ROWS, 2 * HALF), vm(ROWS, 2 * HALF),
            vm(TOK, 2 * HALF), vm(3, HALF, dtype=F32),
            vm(two, HALF, dtype=F32), vm(two, HALF), vm(two, 2 * HALF), vm(3, 8, HALF, dtype=F32),
            vm(D, HALF), vm(D, 2 * HALF),
            vm(4, two, FEAT), vm(4, two, FEAT), vm(4, two, FEAT), vm(6, TOK, FEAT), vm(TOK, FEAT),
        ]
        + wscratch(HALF)
        + wscratch(2 * HALF)
        + [
            vm(8, FEAT, dtype=F32), vm(3, 8, FEAT, dtype=F32), vm(4, 8, FEAT, dtype=F32),
            pltpu.SemaphoreType.DMA((N,)),
            pltpu.SemaphoreType.DMA((N,)),
        ],
        compiler_params=pltpu.CompilerParams(
            collective_id=0, has_side_effects=True, vmem_limit_bytes=67043328
        ),
        name="layer",
    )(
        pre_norm, cotangent, norm_gain[None, :], inputs, down_weight.T,
        gate_weight, value_weight, gate_pre, value_pre, conv_taps,
    )
    return (gi, gg, gv, gd.T, gt, gn[0])


def solution(mesh):
    split = Mesh(mesh.devices.reshape(4, 4, 4, 2), ("z", "y", "x", "c"))
    fs, tp = ("z", "y"), ("x", "c")
    both, across = P(fs, tp), P(tp, fs)
    in_specs = (both, both, both, both, both, both, both, across, P(None, tp), P(tp))
    out_specs = (both, both, both, across, P(None, tp), P(tp))
    return jax.shard_map(on_device, mesh=split, in_specs=in_specs, out_specs=out_specs, check_vma=False)
```

```python
import jax
import jax.numpy as jnp
from jax import lax
from jax.experimental import pallas as pl
from jax.experimental.pallas import tpu as pltpu
from jax.sharding import Mesh
from jax.sharding import PartitionSpec as P

D = 3072
SEQ = 128
EPSILON = 1e-06
HALF = 384
ROWS = 192
TOK = 512
FEAT = 384
BF = jnp.bfloat16
F32 = jnp.float32
MESH = pl.DeviceIdType.MESH


def _mo(v, m):
    return pl.multiple_of(v, m)


class Sems:
    def __init__(self, send, recv):
        self.send, self.recv, self.n, self.all = send, recv, 0, []

    def msg(self, src, dst, **dev):
        i = self.n
        self.n += 1
        m = pltpu.make_async_remote_copy(
            src_ref=src,
            dst_ref=dst,
            send_sem=self.send.at[i],
            recv_sem=self.recv.at[i],
            device_id=dev,
            device_id_type=MESH,
        )
        self.all.append(m)
        return m

    def drain(self):
        for m in self.all:
            m.wait_send()


class Bcast:
    def __init__(self, sems, axis, me, own, slot):
        up, down = lax.rem(me + 1, 4), lax.rem(me + 3, 4)
        to_up, to_down = {axis: up}, {axis: down}
        self.m0 = sems.msg(own(0), slot(me, 0), **to_up)
        self.m1 = sems.msg(own(1), slot(me, 1), **to_down)
        self.m2 = sems.msg(own(1), slot(me, 1), **to_up)
        self.m3 = sems.msg(own(0), slot(me, 0), **to_down)
        self.m4 = sems.msg(slot(down, 0), slot(down, 0), **to_up)
        self.m5 = sems.msg(slot(up, 1), slot(up, 1), **to_down)

    def f0(self):
        self.m0.wait_recv()
        self.m4.start()

    def f1(self):
        self.m1.wait_recv()
        self.m5.start()

    def near(self):
        self.m2.wait_recv()
        self.m3.wait_recv()

    def far(self):
        self.m4.wait_recv()
        self.m5.wait_recv()


class Scatter:
    def __init__(self, sems, axis, me, chunk, got, rows, step):
        up, down = lax.rem(me + 1, 4), lax.rem(me + 3, 4)
        far = lax.rem(me + 2, 4)
        to_up, to_down = {axis: up}, {axis: down}
        self.me, self.up, self.down = me, up, down
        self.chunk, self.got, self.rows, self.step = chunk, got, rows, step
        self.m0 = sems.msg(chunk(far, 0), got.at[0], **to_up)
        self.m1 = sems.msg(chunk(far, 1), got.at[1], **to_down)
        self.m2 = sems.msg(chunk(up, 1), got.at[2], **to_up)
        self.m3 = sems.msg(chunk(down, 0), got.at[3], **to_down)
        self.m4 = sems.msg(chunk(up, 0), got.at[4], **to_up)
        self.m5 = sems.msg(chunk(down, 1), got.at[5], **to_down)

    def g0(self):
        self.m0.wait_recv()
        add_to(self.chunk(self.up, 0), self.got.at[0], self.rows, self.step)
        self.m4.start()

    def g1(self):
        self.m1.wait_recv()
        add_to(self.chunk(self.down, 1), self.got.at[1], self.rows, self.step)
        self.m5.start()

    def last(self, h, put):
        a, b = ((3, 4), (2, 5))[h]
        (self.m3, self.m2)[h].wait_recv()
        (self.m4, self.m5)[h].wait_recv()
        n = self.step
        own = self.chunk(self.me, h)

        @pl.loop(0, self.rows // n)
        def _(i):
            r = pl.ds(_mo(i * n, 16), n)
            put(h, i * n, n, own[r, :].astype(F32) + self.got[a, r, :].astype(F32) + self.got[b, r, :].astype(F32))


def add_to(dst, src, rows, step):
    @pl.loop(0, rows // step)
    def _(i):
        r = pl.ds(_mo(i * step, 16), step)
        dst[r, :] = (dst[r, :].astype(F32) + src[r, :].astype(F32)).astype(BF)


def mm(a, b, ca, cb):
    return lax.dot_general(a, b, (((ca,), (cb,)), ((), ())), preferred_element_type=F32)


def kernel(
    pre, cot, gain, xin_hbm, down_hbm, gatew_hbm, valuew_hbm, gatep, valuep, taps,
    *refs,
):
    results, scratch = refs[:6], refs[6:]
    (
        GP, X, Wd, Wg, PRE, st, gpo, wdm,
        wdt, wgm, wgt, pt, tap, saved, xin, down,
        gatew, valuew, gi, gg_out, gv_out, gd_out, gt_out, gn_out,
        GA, hid, G, tacc, Dd, Dg, CS, MC,
        E, xgot, xlin, dgot, dhb, dhq, dlin, ggot,
        ghb, ghq, glin, small, sz, sy, ss, rs,
        ls,
    ) = scratch
    z, y = lax.axis_index("z"), lax.axis_index("y")
    x, c = lax.axis_index("x"), lax.axis_index("c")
    yp = y + 1 - 2 * lax.rem(y, 2)
    yh = 3 - y
    yq = yh + 1 - 2 * lax.rem(yh, 2)
    hs = lax.rem((y + 1) // 2, 2)
    sib = 1 - c
    tp = x * 2 + c
    zk = [lax.rem(z + k, 4) for k in range(4)]
    xk = [lax.rem(x + k, 4) for k in range(4)]
    sems = Sems(ss, rs)
    hbm = (down_hbm, xin_hbm, gatew_hbm, valuew_hbm, gatep, valuep)
    here = (down, xin, gatew, valuew, saved.at[0], saved.at[1])
    loads = [pltpu.make_async_copy(a, b, ls.at[k]) for k, (a, b) in enumerate(zip(hbm, here))]
    for m in loads:
        m.start()
    found = (gi, gg_out, gv_out, gd_out, gt_out, gn_out)
    stores = [pltpu.make_async_copy(a, b, ls.at[6 + k]) for k, (a, b) in enumerate(zip(found, results))]

    barrier = pltpu.get_barrier_semaphore()
    peers = [{"z": zk[1]}, {"z": zk[2]}, {"z": zk[3]}, {"y": yp}, {"y": yh}, {"y": yq}]
    tps = []
    for k in range(1, 8):
        t = lax.rem(tp + k, 8)
        tps.append({"x": t // 2, "c": lax.rem(t, 2)})
    for dev in peers + tps:
        pl.semaphore_signal(barrier, inc=1, device_id=dev, device_id_type=MESH)

    def lane_sums(v):
        v = v[:, :128] + v[:, 128:256] + v[:, 256:384]
        return jnp.sum(v.T, axis=0, keepdims=True)

    pf = pre[...].astype(F32)
    cf = cot[...].astype(F32)
    scaled = gain[...][None, :] * cf
    for j, v in enumerate((lane_sums(pf * pf), lane_sums(pf * scaled))):
        for i in range(4):
            st[0, j * 4 + i : j * 4 + i + 1, :] = v[:, i * 128 : (i + 1) * 128]

    def split(src, mine, theirs):
        n = src.shape[0]
        rest = src.shape[1] - HALF
        fill = jnp.zeros((n, HALF - rest), src.dtype)

        @pl.when(hs == 0)
        def _():
            mine[...] = src[:, :HALF]
            if theirs is not None:
                theirs[:, :rest] = src[:, HALF:]
                theirs[:, rest:] = fill

        @pl.when(hs == 1)
        def _():
            mine[:, :rest] = src[:, HALF:]
            mine[:, rest:] = fill
            if theirs is not None:
                theirs[...] = src[:, :HALF]

    loads[0].wait()
    split(down, wdm, wdt)
    loads[1].wait()

    def split_rows(src, mine, theirs):
        rest = src.shape[0] - HALF
        fill = jnp.zeros((HALF - rest, src.shape[1]), src.dtype)

        @pl.when(hs == 0)
        def _():
            mine[...] = src[:HALF]
            theirs[:rest] = src[HALF:]
            theirs[rest:] = fill

        @pl.when(hs == 1)
        def _():
            mine[:rest] = src[HALF:]
            mine[rest:] = fill
            theirs[...] = src[:HALF]

    class Gather:
        def __init__(self, mine, theirs, buf):
            def rows(zz, yy, h=None):
                if h is None:
                    return buf.at[pl.ds(_mo((zz * 4 + yy) * ROWS, 16), ROWS)]
                return buf.at[pl.ds(_mo((zz * 4 + yy) * ROWS + h * 96, 16), 96)]

            self.b0 = Bcast(
                sems, "z", z, lambda h: mine.at[pl.ds(h * 96, 96)], lambda zz, h: rows(zz, y, h)
            )
            self.lo = sems.msg(theirs, rows(z, y), y=yp)
            zs = [zk[0], zk[3], zk[1], zk[2]]
            self.u = [sems.msg(mine if k == 0 else rows(zz, y), rows(zz, y), y=yh) for k, zz in enumerate(zs)]
            self.u4 = sems.msg(rows(z, yp), rows(z, yp), y=yh)
            self.b1 = Bcast(sems, "z", z, lambda h: rows(z, yp, h), lambda zz, h: rows(zz, yp, h))
            self.b2 = Bcast(sems, "z", z, lambda h: rows(z, yq, h), lambda zz, h: rows(zz, yq, h))
            self.mine, self.buf = mine, buf

        def keep(self):
            self.buf[pl.ds(_mo((z * 4 + y) * ROWS, 16), ROWS), :] = self.mine[...]

        def n1(self):
            self.b0.m2.wait_recv()
            self.u[1].start()

        def n2(self):
            self.b0.m3.wait_recv()
            self.u[2].start()

        def far(self):
            self.b0.far()
            self.u[3].start()

        def arrived(self):
            self.b1.near()
            self.b1.far()
            self.b2.near()
            self.b2.far()
            for m in self.u:
                m.wait_recv()

    class Acts:
        def __init__(self, own, buf, kind):
            def slot(xx, h=None):
                lanes = pl.ds(_mo((xx * 2 + c) * FEAT, 128), FEAT)
                if h is None:
                    return buf.at[pl.ds(kind * TOK, TOK), lanes]
                return buf.at[pl.ds(kind * TOK + h * 256, 256), lanes]

            half = (lambda h: own.at[pl.ds(h * 256, 256)]) if kind == 0 else (lambda h: slot(x, h))
            self.b = Bcast(sems, "x", x, half, slot)
            xs = [xk[0], xk[3], xk[1], xk[2]]
            self.d = [
                sems.msg(own if (k == 0 and kind == 0) else slot(xx), slot(xx), c=sib)
                for k, xx in enumerate(xs)
            ]
            if kind == 0:
                lanes = pl.ds(_mo(tp * FEAT, 128), FEAT)
                self.lo = sems.msg(own, buf.at[pl.ds(TOK, TOK), lanes], y=yp)

        def n1(self):
            self.b.m2.wait_recv()
            self.d[1].start()

        def n2(self):
            self.b.m3.wait_recv()
            self.d[2].start()

        def far(self):
            self.b.far()
            self.d[3].start()

        def arrived(self):
            for m in self.d:
                m.wait_recv()

    class Reduce:
        def __init__(self, src, got, hb, hq, lin):
            def rows(zz, yy, h=None):
                if h is None:
                    return src.at[pl.ds(_mo((zz * 4 + yy) * ROWS, 16), ROWS)]
                return src.at[pl.ds(_mo((zz * 4 + yy) * ROWS + h * 96, 16), 96)]

            self.rows, self.hb, self.hq, self.lin = rows, hb, hq, lin
            self.zq = Scatter(sems, "z", z, lambda zz, h: rows(zz, yq, h), got.at[0], 96, 48)
            self.zp = Scatter(sems, "z", z, lambda zz, h: rows(zz, yp, h), got.at[1], 96, 48)
            self.zo = Scatter(sems, "z", z, lambda zz, h: rows(zz, y, h), got.at[2], 96, 48)
            self.v = [sems.msg(rows(zk[k], yh), hb.at[k], y=yh) for k in range(4)]
            half = [pl.ds(0, 96), pl.ds(96, 96)]
            self.w = [sems.msg(rows(z, yq, h), hq.at[half[h]], y=yh) for h in (0, 1)]
            self.l = [sems.msg(rows(z, yp, h), lin.at[half[h]], y=yp) for h in (0, 1)]

        def merge_hi(self, k):
            self.v[k].wait_recv()
            add_to(self.rows(zk[k], y), self.hb.at[k], ROWS, 48)

        def q(self, h):
            own = self.rows(z, yq)

            def put(h, i, n, total):
                own[pl.ds(_mo(h * 96 + i, 16), n), :] = total.astype(BF)

            self.zq.last(h, put)
            self.w[h].start()

        def p(self, h):
            self.w[h].wait_recv()
            own = self.rows(z, yp)

            def put(h, i, n, total):
                r = pl.ds(_mo(h * 96 + i, 16), n)
                own[r, :] = (total + self.hq[r, :].astype(F32)).astype(BF)

            self.zp.last(h, put)
            self.l[h].start()

        def o(self, h, outs):
            def put(h, i, n, total):
                write(outs, hs, h * 96 + i, n, total)

            self.zo.last(h, put)

        def t(self, h, outs):
            self.l[h].wait_recv()

            @pl.loop(0, 2)
            def _(i):
                at = _mo(h * 96 + i * 48, 16)
                write(outs, 1 - hs, at, 48, self.lin[pl.ds(at, 48), :].astype(F32))

    def write(outs, half, row, n, value):
        r = pl.ds(_mo(row, 16), n)
        for j, out in enumerate(outs):
            part = value[:, j * HALF : (j + 1) * HALF]
            rest = out.shape[1] - HALF

            @pl.when(half == 0)
            def _():
                out[r, :HALF] = part

            @pl.when(half == 1)
            def _():
                out[r, HALF:] = part[:, :rest]

    gd = Gather(wdm, wdt, Wd)
    gw = Gather(wgm, wgt, Wg)
    go, gp = Acts(gpo, GP, 0), Acts(None, GP, 1)
    xo, xp = Acts(xin, X, 0), Acts(None, X, 1)
    plo = sems.msg(pt, PRE.at[:, pl.ds(TOK, TOK)], y=yp)
    stats = [sems.msg(st.at[0], st.at[k], **tps[k - 1]) for k in range(1, 8)]
    sd = Reduce(Dd, dgot, dhb, dhq, dlin)
    sw = Reduce(Dg, ggot, ghb, ghq, glin)
    e = [sems.msg(CS.at[k], E.at[k], c=sib) for k in range(4)]
    xs = Scatter(sems, "x", x, lambda xx, h: MC.at[lax.rem(xx - x + 4, 4), pl.ds(h * TOK, TOK)], xgot, TOK, 64)
    xl = sems.msg(MC.at[0, pl.ds(TOK, TOK)], xlin, y=yp)
    sz_m = [sems.msg(small, sz.at[k - 1], z=zk[k]) for k in (1, 2, 3)]
    sy_m = [sems.msg(sy.at[3], sy.at[k], y=yy) for k, yy in enumerate((yh, yp, yq))]

    def grad_act(kind):
        @pl.loop(0, 2)
        def _(i):
            r = pl.ds(_mo(kind * TOK + i * 256, 256), 256)
            GA[r, :] = mm(GP[r, :], Wd[...], 1, 0)

    def middle(kind, lo, hi):
        row = lax.broadcasted_iota(jnp.int32, (SEQ, 128), 0)

        def prev(v):
            return jnp.where(row == 0, 0.0, pltpu.roll(v, 1, 0))

        def succ(v):
            return jnp.where(row == SEQ - 1, 0.0, pltpu.roll(v, SEQ - 1, 0))

        @pl.loop(lo, hi)
        def _(i):
            r = pl.ds(_mo(kind * TOK + (i // 3) * SEQ, SEQ), SEQ)
            at = lax.rem(i, 3) * 128
            lanes, lanes2 = pl.ds(_mo(at, 128), 128), pl.ds(_mo(HALF + at, 128), 128)
            gate = PRE[lanes, r].astype(F32).T
            value = PRE[lanes2, r].astype(F32).T
            t0, t1, t2 = (tap[k : k + 1, lanes] for k in range(3))
            before, after = prev(gate), succ(gate)
            mixed = t0 * before + t1 * gate + t2 * after
            sig = jax.nn.sigmoid(mixed)
            active = mixed * sig
            ga = GA[r, lanes]
            hid[r, lanes] = (active * value).astype(BF)
            G[r, lanes2] = (ga * active).astype(BF)
            gm = ga * value * sig * (1.0 + mixed * (1.0 - sig))
            G[r, lanes] = (t1 * gm + t0 * succ(gm) + t2 * prev(gm)).astype(BF)
            for k, v in enumerate((before, gate, after)):
                tacc[k, :, lanes] += jnp.sum((gm * v).reshape(SEQ // 8, 8, 128), axis=0)

    def block(dst, left, right, zz, yy):
        at = _mo((zz * 2 + yy // 2) * FEAT, 128)
        dst[pl.ds(at, FEAT), :] = mm(left[:, pl.ds(at, FEAT)], right[...], 0, 0).astype(BF)

    def blocks(dst, left, right, yy, first):
        @pl.loop(0, 2)
        def _(k):
            zz = lax.rem(z + 2 - k + 4, 4) if first else lax.rem(z + 3 + k, 4)
            block(dst, left, right, zz, yy)

    def contrib(dst, cc, first):
        @pl.loop(0, 2)
        def _(i):
            k = 2 - i if first else lax.rem(3 + i, 4)
            at = _mo((lax.rem(x + k, 4) * 2 + cc) * FEAT, 128)
            dst[k] = mm(G[...], Wg[pl.ds(at, FEAT), :], 1, 1).astype(BF)

    pl.semaphore_wait(barrier, 13)
    for m in stats:
        m.start()
    gd.b0.m0.start()
    gd.b0.m1.start()
    gd.u[0].start()
    gd.lo.start()
    xo.b.m0.start()
    xo.b.m1.start()
    gd.b0.m2.start()
    gd.b0.m3.start()
    xo.d[0].start()
    own_lanes = pl.ds(_mo(tp * FEAT, 128), FEAT)
    X[0:TOK, own_lanes] = xin[...]
    gd.keep()
    split(taps, tap, None)
    tacc[...] = jnp.zeros_like(tacc)
    for m in loads[2:4]:
        m.wait()
    split(gatew, wgm.at[:, 0:HALF], wgt.at[:, 0:HALF])
    split(valuew, wgm.at[:, HALF : 2 * HALF], wgt.at[:, HALF : 2 * HALF])
    gw.keep()
    gw.b0.m0.start()
    gw.u[0].start()
    gw.b0.m3.start()
    gw.b0.m2.start()
    gw.b0.m1.start()
    for m in stats:
        m.wait_recv()
    tot = st[0]
    for k in range(1, 8):
        tot = tot + st[k]
    inverse = lax.rsqrt(tot[0:4] / D + EPSILON)
    coef = inverse * inverse * (tot[4:8] / D)

    def column(v):
        v = jnp.concatenate([jnp.broadcast_to(v[i : i + 1], (128, 128)).T for i in range(4)], axis=0)
        return jnp.concatenate([v, v, v], axis=1)

    inv = column(inverse)
    pf = pre[...].astype(F32)
    cf = cot[...].astype(F32)
    scaled = gain[...][None, :] * cf
    g = (inv * (scaled - pf * column(coef))).astype(BF)
    gpo[...] = g
    GP[0:TOK, own_lanes] = g
    small[...] = jnp.broadcast_to(jnp.sum(cf * pf * inv, axis=0, keepdims=True), (8, FEAT))
    go.lo.start()
    go.b.m0.start()
    go.b.m1.start()
    go.b.m3.start()
    go.d[0].start()
    go.b.m2.start()
    gw.lo.start()
    for m in loads[4:]:
        m.wait()
    split_rows(saved.at[0], PRE.at[0:HALF, 0:TOK], pt.at[0:HALF])
    split_rows(saved.at[1], PRE.at[HALF : 2 * HALF, 0:TOK], pt.at[HALF : 2 * HALF])

    gd.b0.f0()
    xo.lo.start()
    gd.lo.wait_recv()
    gd.b1.m1.start()
    gd.b1.m2.start()
    gd.u4.start()
    gd.b1.m0.start()
    gd.b1.m3.start()
    gd.b0.f1()
    gd.n2()
    gw.b0.f0()
    go.b.f1()
    go.b.f0()
    gd.b1.f1()
    gw.n1()
    go.lo.wait_recv()
    gp.d[0].start()
    gp.b.m0.start()
    gp.b.m3.start()
    gp.b.m2.start()
    gp.b.m1.start()
    gw.b0.f1()
    gd.n1()
    go.n2()
    xo.b.m2.start()
    xo.b.m3.start()
    xo.b.f1()
    xo.b.f0()
    gd.u4.wait_recv()
    gd.b2.m0.start()
    gd.b2.m1.start()
    gd.b2.m3.start()
    gd.b2.m2.start()
    go.n1()
    gd.far()
    gd.b1.f0()
    go.far()
    gw.lo.wait_recv()
    gw.b1.m1.start()
    gw.b1.m2.start()
    gw.u4.start()
    gw.b1.m3.start()
    gw.b1.m0.start()
    gw.n2()
    gd.b2.f0()
    gw.far()
    gd.b2.f1()
    go.arrived()
    plo.start()
    gp.b.f0()
    gp.b.f1()
    gw.b1.f1()
    gp.n2()
    gp.n1()
    xo.lo.wait_recv()
    xp.b.m0.start()
    xp.b.m1.start()
    xp.b.m2.start()
    xp.d[0].start()
    xp.b.m3.start()
    gw.b1.f0()
    xo.n2()
    gd.arrived()
    grad_act(0)
    middle(0, 0, 6)
    middle(0, 6, 12)
    gw.u4.wait_recv()
    gw.b2.m1.start()
    gw.b2.m0.start()
    gw.b2.m3.start()
    gw.b2.m2.start()
    gp.far()
    gw.b2.f0()
    gw.b2.f1()
    gp.arrived()
    grad_act(1)
    xo.n1()
    xp.b.f0()
    xp.b.f1()
    xo.far()
    plo.wait_recv()
    middle(1, 0, 6)
    middle(1, 6, 12)
    blocks(Dd, GP, hid, yh, True)
    sd.zq.m0.start()
    sd.zq.m2.start()
    sd.v[2].start()
    sd.v[1].start()
    sd.zq.m1.start()
    xp.n2()
    for k in range(3):
        small[k : k + 1, :] = jnp.sum(tacc[k], axis=0, keepdims=True)
    for m in sz_m:
        m.start()
    gw.arrived()
    contrib(CS, sib, True)
    e[2].start()
    e[1].start()
    xo.arrived()
    xp.n1()
    blocks(Dd, GP, hid, yh, False)
    sd.zq.m3.start()
    sd.v[3].start()
    sd.v[0].start()
    blocks(Dd, GP, hid, y, True)
    sd.zp.m0.start()
    sd.zp.m1.start()
    sd.zp.m2.start()
    xp.far()
    sd.zq.g1()
    contrib(CS, sib, False)
    e[3].start()
    e[0].start()
    contrib(MC, c, True)
    e[2].wait_recv()
    add_to(MC.at[2], E.at[2], 2 * TOK, 64)
    xs.m1.start()
    xs.m0.start()
    sd.zq.g0()
    contrib(MC, c, False)
    sd.q(1)
    xp.arrived()
    blocks(Dg, X, G, yh, True)
    sw.v[1].start()
    sw.zq.m0.start()
    sw.v[2].start()
    sw.zq.m1.start()
    sw.zq.m2.start()
    sd.q(0)
    blocks(Dg, X, G, yh, False)
    sw.zq.m3.start()
    sw.v[3].start()
    sw.v[0].start()
    e[1].wait_recv()
    add_to(MC.at[1], E.at[1], 2 * TOK, 64)
    xs.m2.start()
    e[3].wait_recv()
    add_to(MC.at[3], E.at[3], 2 * TOK, 64)
    xs.m3.start()
    e[0].wait_recv()
    add_to(MC.at[0], E.at[0], 2 * TOK, 64)

    sw.zq.g0()
    sw.zq.g1()
    xs.g0()
    blocks(Dd, GP, hid, y, False)
    sd.zp.m3.start()
    sd.zp.g1()
    xs.g1()
    sd.merge_hi(2)
    sd.zo.m1.start()
    sd.zo.m0.start()
    sd.merge_hi(1)
    sd.zo.m2.start()
    sd.merge_hi(3)
    sd.zo.m3.start()
    sd.zp.g0()
    sd.merge_hi(0)

    sw.q(1)
    blocks(Dg, X, G, y, True)
    sw.zp.m1.start()
    sw.zp.m0.start()
    sw.zp.m2.start()
    sd.p(1)
    blocks(Dg, X, G, y, False)
    sw.zp.m3.start()
    sd.zo.g1()
    sd.p(0)
    sd.t(1, (gd_out,))
    sw.zp.g0()
    sw.q(0)
    sd.t(0, (gd_out,))
    sw.merge_hi(2)
    sw.zo.m1.start()
    sw.zo.m0.start()
    sw.merge_hi(1)
    sw.zo.m2.start()
    sw.zp.g1()
    sd.zo.g0()
    sw.merge_hi(3)
    sw.zo.m3.start()
    def put1(h, i, n, total):
        MC[0, pl.ds(_mo(TOK + i, 16), n), :] = total.astype(BF)

    xs.last(1, put1)
    xl.start()
    def put0(h, i, n, total):
        GA[pl.ds(_mo(i, 16), n), :] = total

    xs.last(0, put0)
    sd.o(1, (gd_out,))
    sw.zo.g1()
    sw.zo.g0()
    sw.merge_hi(0)

    sw.p(1)
    sd.o(0, (gd_out,))
    stores[3].start()
    for m in sz_m:
        m.wait_recv()
    sy[3] = small[...] + sz[0] + sz[1] + sz[2]
    for m in sy_m:
        m.start()
    xl.wait_recv()

    @pl.loop(0, 8)
    def _(i):
        r = pl.ds(_mo(i * 64, 16), 64)
        gi[r, :] = (GA[r, :] + xlin[r, :].astype(F32)).astype(BF)

    stores[0].start()
    sw.p(0)
    for m in sy_m:
        m.wait_recv()
    rest = gt_out.shape[1] - HALF
    mine_sum = sy[3] + sy[0]
    their_sum = sy[1] + sy[2]

    @pl.when(hs == 0)
    def _():
        gt_out[:, :HALF] = mine_sum[0:3]
        gt_out[:, HALF:] = their_sum[0:3, :rest]

    @pl.when(hs == 1)
    def _():
        gt_out[:, :HALF] = their_sum[0:3]
        gt_out[:, HALF:] = mine_sum[0:3, :rest]

    gn_out[...] = (mine_sum[3:4] + their_sum[3:4])[0]
    stores[4].start()
    stores[5].start()
    sw.o(0, (gg_out, gv_out))
    sw.t(1, (gg_out, gv_out))
    sw.o(1, (gg_out, gv_out))
    sw.t(0, (gg_out, gv_out))
    stores[1].start()
    stores[2].start()
    for m in stores:
        m.wait()
    sems.drain()


N = 7 + 2 * 24 + 4 * 10 + 2 + 1 + 2 * 26 + 4 + 6 + 1 + 6
VM = pl.BlockSpec(memory_space=pltpu.VMEM)
ANY = pl.BlockSpec(memory_space=pl.ANY)


def hand_on(*refs):
    src, dst, here = refs[:6], refs[6:12], refs[12:18]
    took = [pltpu.make_async_copy(a, b, refs[18].at[k]) for k, (a, b) in enumerate(zip(src, here))]
    gave = [pltpu.make_async_copy(a, b, refs[19].at[k]) for k, (a, b) in enumerate(zip(here, dst))]
    for m in took:
        m.start()
    for k in (1, 2, 3, 0, 4, 5):
        took[k].wait()
        gave[k].start()
    for m in gave:
        m.wait()


def on_device(
    inputs, cotangent, pre_norm, gate_pre, value_pre, gate_weight, value_weight, down_weight, conv_taps, norm_gain
):
    width = gate_pre.shape[1]

    def vm(*shape, dtype=BF):
        return pltpu.VMEM(shape, dtype)

    def wscratch(n):
        return [vm(3, 6, 96, n), vm(4, ROWS, n), vm(ROWS, n), vm(ROWS, n)]

    two = 2 * TOK
    outs = pl.pallas_call(
        kernel,
        out_shape=(
            jax.ShapeDtypeStruct((TOK, FEAT), BF),
            jax.ShapeDtypeStruct((ROWS, width), F32),
            jax.ShapeDtypeStruct((ROWS, width), F32),
            jax.ShapeDtypeStruct((ROWS, width), F32),
            jax.ShapeDtypeStruct((3, width), F32),
            jax.ShapeDtypeStruct((FEAT,), F32),
        ),
        in_specs=[VM] * 3 + [ANY] * 6 + [VM],
        out_specs=(ANY,) * 6,
        scratch_shapes=[
            vm(two, D), vm(two, D), vm(D, HALF), vm(D, 2 * HALF), vm(2 * HALF, two),
            vm(8, 8, 128, dtype=F32), vm(TOK, FEAT),
            vm(ROWS, HALF), vm(ROWS, HALF), vm(ROWS, 2 * HALF), vm(ROWS, 2 * HALF),
            vm(2 * HALF, TOK), vm(3, HALF, dtype=F32), vm(2, width, TOK),
            vm(TOK, FEAT), vm(ROWS, width), vm(ROWS, width), vm(ROWS, width),
            vm(TOK, FEAT), vm(ROWS, width, dtype=F32), vm(ROWS, width, dtype=F32), vm(ROWS, width, dtype=F32),
            vm(3, width, dtype=F32), vm(FEAT, dtype=F32),
            vm(two, HALF, dtype=F32), vm(two, HALF), vm(two, 2 * HALF), vm(3, 8, HALF, dtype=F32),
            vm(D, HALF), vm(D, 2 * HALF),
            vm(4, two, FEAT), vm(4, two, FEAT), vm(4, two, FEAT), vm(6, TOK, FEAT), vm(TOK, FEAT),
        ]
        + wscratch(HALF)
        + wscratch(2 * HALF)
        + [
            vm(8, FEAT, dtype=F32), vm(3, 8, FEAT, dtype=F32), vm(4, 8, FEAT, dtype=F32),
            pltpu.SemaphoreType.DMA((N,)),
            pltpu.SemaphoreType.DMA((N,)),
            pltpu.SemaphoreType.DMA((12,)),
        ],
        compiler_params=pltpu.CompilerParams(
            collective_id=0, has_side_effects=True, vmem_limit_bytes=67043328
        ),
        name="layer",
    )(
        pre_norm, cotangent, norm_gain, inputs, down_weight.T,
        gate_weight, value_weight, gate_pre.T, value_pre.T, conv_taps,
    )
    outs = pl.pallas_call(
        hand_on,
        out_shape=tuple(jax.ShapeDtypeStruct(a.shape, a.dtype) for a in outs),
        in_specs=[ANY] * 6,
        out_specs=(ANY,) * 6,
        scratch_shapes=[pltpu.VMEM(a.shape, a.dtype) for a in outs]
        + [pltpu.SemaphoreType.DMA((6,)), pltpu.SemaphoreType.DMA((6,))],
        name="hand_on",
    )(*outs)
    gi, gg, gv, gd, gt, gn = outs
    return (gi, gg, gv, gd.T, gt, gn)


def solution(mesh):
    split = Mesh(mesh.devices.reshape(4, 4, 4, 2), ("z", "y", "x", "c"))
    fs, tp = ("z", "y"), ("x", "c")
    both, across = P(fs, tp), P(tp, fs)
    in_specs = (both, both, both, both, both, both, both, across, P(None, tp), P(tp))
    out_specs = (both, both, both, across, P(None, tp), P(tp))
    return jax.shard_map(on_device, mesh=split, in_specs=in_specs, out_specs=out_specs, check_vma=False)
```

```python
import jax
import jax.numpy as jnp
from jax import lax
from jax.experimental import pallas as pl
from jax.experimental.pallas import tpu as pltpu
from jax.sharding import Mesh
from jax.sharding import PartitionSpec as P

D = 3072
SEQ = 128
EPSILON = 1e-06
HALF = 384
ROWS = 192
TOK = 512
FEAT = 384
BF = jnp.bfloat16
F32 = jnp.float32
MESH = pl.DeviceIdType.MESH


def _mo(v, m):
    return pl.multiple_of(v, m)


class Sems:
    def __init__(self, send, recv):
        self.send, self.recv, self.n, self.all = send, recv, 0, []

    def msg(self, src, dst, **dev):
        i = self.n
        self.n += 1
        m = pltpu.make_async_remote_copy(
            src_ref=src,
            dst_ref=dst,
            send_sem=self.send.at[i],
            recv_sem=self.recv.at[i],
            device_id=dev,
            device_id_type=MESH,
        )
        self.all.append(m)
        return m

    def drain(self):
        for m in self.all:
            m.wait_send()


class Bcast:
    def __init__(self, sems, axis, me, own, slot):
        up, down = lax.rem(me + 1, 4), lax.rem(me + 3, 4)
        to_up, to_down = {axis: up}, {axis: down}
        self.m0 = sems.msg(own(0), slot(me, 0), **to_up)
        self.m1 = sems.msg(own(1), slot(me, 1), **to_down)
        self.m2 = sems.msg(own(1), slot(me, 1), **to_up)
        self.m3 = sems.msg(own(0), slot(me, 0), **to_down)
        self.m4 = sems.msg(slot(down, 0), slot(down, 0), **to_up)
        self.m5 = sems.msg(slot(up, 1), slot(up, 1), **to_down)

    def f0(self):
        self.m0.wait_recv()
        self.m4.start()

    def f1(self):
        self.m1.wait_recv()
        self.m5.start()

    def near(self):
        self.m2.wait_recv()
        self.m3.wait_recv()

    def far(self):
        self.m4.wait_recv()
        self.m5.wait_recv()


class Scatter:
    def __init__(self, sems, axis, me, chunk, got, rows, step):
        up, down = lax.rem(me + 1, 4), lax.rem(me + 3, 4)
        far = lax.rem(me + 2, 4)
        to_up, to_down = {axis: up}, {axis: down}
        self.me, self.up, self.down = me, up, down
        self.chunk, self.got, self.rows, self.step = chunk, got, rows, step
        self.m0 = sems.msg(chunk(far, 0), got.at[0], **to_up)
        self.m1 = sems.msg(chunk(far, 1), got.at[1], **to_down)
        self.m2 = sems.msg(chunk(up, 1), got.at[2], **to_up)
        self.m3 = sems.msg(chunk(down, 0), got.at[3], **to_down)
        self.m4 = sems.msg(chunk(up, 0), got.at[4], **to_up)
        self.m5 = sems.msg(chunk(down, 1), got.at[5], **to_down)

    def g0(self):
        self.m0.wait_recv()
        add_to(self.chunk(self.up, 0), self.got.at[0], self.rows, self.step)
        self.m4.start()

    def g1(self):
        self.m1.wait_recv()
        add_to(self.chunk(self.down, 1), self.got.at[1], self.rows, self.step)
        self.m5.start()

    def last(self, h, put):
        a, b = ((3, 4), (2, 5))[h]
        (self.m3, self.m2)[h].wait_recv()
        (self.m4, self.m5)[h].wait_recv()
        n = self.step
        own = self.chunk(self.me, h)

        @pl.loop(0, self.rows // n)
        def _(i):
            r = pl.ds(_mo(i * n, 16), n)
            put(h, i * n, n, own[r, :].astype(F32) + self.got[a, r, :].astype(F32) + self.got[b, r, :].astype(F32))


def add_to(dst, src, rows, step):
    @pl.loop(0, rows // step)
    def _(i):
        r = pl.ds(_mo(i * step, 16), step)
        dst[r, :] = (dst[r, :].astype(F32) + src[r, :].astype(F32)).astype(BF)


def mm(a, b, ca, cb):
    return lax.dot_general(a, b, (((ca,), (cb,)), ((), ())), preferred_element_type=F32)


def kernel(
    pre, cot, gain, xin_hbm, down_hbm, gatew_hbm, valuew_hbm, gatep, valuep, taps,
    *refs,
):
    results, scratch = refs[:6], refs[6:]
    (
        GP, X, Wd, Wg, PRE, st, gpo, wdm,
        wdt, wgm, wgt, pt, tap, saved, tgot, tin, xin, down,
        gatew, valuew, gi, gg_out, gv_out, gd_out, gt_out, gn_out,
        GA, hid, G, tacc, Dd, Dg, CS, MC,
        E, xgot, xlin, dgot, dhb, dhq, dlin, ggot,
        ghb, ghq, glin, small, sz, sy, ss, rs,
        ls,
    ) = scratch
    z, y = lax.axis_index("z"), lax.axis_index("y")
    x, c = lax.axis_index("x"), lax.axis_index("c")
    yp = y + 1 - 2 * lax.rem(y, 2)
    yh = 3 - y
    yq = yh + 1 - 2 * lax.rem(yh, 2)
    hs = lax.rem((y + 1) // 2, 2)
    sib = 1 - c
    tp = x * 2 + c
    zk = [lax.rem(z + k, 4) for k in range(4)]
    xk = [lax.rem(x + k, 4) for k in range(4)]
    sems = Sems(ss, rs)
    hbm = (down_hbm, xin_hbm, gatew_hbm, valuew_hbm, gatep, valuep)
    here = (down, xin, gatew, valuew, saved.at[0], saved.at[1])
    loads = [pltpu.make_async_copy(a, b, ls.at[k]) for k, (a, b) in enumerate(zip(hbm, here))]
    for m in loads:
        m.start()
    found = (gi, gg_out, gv_out, gd_out, gt_out, gn_out)
    stores = [pltpu.make_async_copy(a, b, ls.at[6 + k]) for k, (a, b) in enumerate(zip(found, results))]

    barrier = pltpu.get_barrier_semaphore()
    peers = [{"z": zk[1]}, {"z": zk[2]}, {"z": zk[3]}, {"y": yp}, {"y": yh}, {"y": yq}]
    tps = []
    for k in range(1, 8):
        t = lax.rem(tp + k, 8)
        tps.append({"x": t // 2, "c": lax.rem(t, 2)})
    for dev in peers + tps:
        pl.semaphore_signal(barrier, inc=1, device_id=dev, device_id_type=MESH)

    def lane_sums(v):
        v = v[:, :128] + v[:, 128:256] + v[:, 256:384]
        return jnp.sum(v.T, axis=0, keepdims=True)

    pf = pre[...].astype(F32)
    cf = cot[...].astype(F32)
    scaled = gain[...][None, :] * cf
    for j, v in enumerate((lane_sums(pf * pf), lane_sums(pf * scaled))):
        for i in range(4):
            st[0, j * 4 + i : j * 4 + i + 1, :] = v[:, i * 128 : (i + 1) * 128]

    def split(src, mine, theirs):
        n = src.shape[0]
        rest = src.shape[1] - HALF
        fill = jnp.zeros((n, HALF - rest), src.dtype)

        @pl.when(hs == 0)
        def _():
            mine[...] = src[:, :HALF]
            if theirs is not None:
                theirs[:, :rest] = src[:, HALF:]
                theirs[:, rest:] = fill

        @pl.when(hs == 1)
        def _():
            mine[:, :rest] = src[:, HALF:]
            mine[:, rest:] = fill
            if theirs is not None:
                theirs[...] = src[:, :HALF]

    loads[0].wait()
    split(down, wdm, wdt)
    loads[1].wait()

    def split_rows(src, mine, theirs):
        rest = src.shape[0] - HALF
        fill = jnp.zeros((HALF - rest, src.shape[1]), src.dtype)

        @pl.when(hs == 0)
        def _():
            mine[...] = src[:HALF]
            theirs[:rest] = src[HALF:]
            theirs[rest:] = fill

        @pl.when(hs == 1)
        def _():
            mine[:rest] = src[HALF:]
            mine[rest:] = fill
            theirs[...] = src[:HALF]

    class Gather:
        def __init__(self, mine, theirs, buf, tail=0):
            def rows(zz, yy, h=None):
                if h is None:
                    return buf.at[pl.ds(_mo((zz * 4 + yy) * ROWS, 16), ROWS)]
                return buf.at[pl.ds(_mo((zz * 4 + yy) * ROWS + h * 96, 16), 96)]

            self.b0 = Bcast(
                sems, "z", z, lambda h: mine.at[pl.ds(h * 96, 96)], lambda zz, h: rows(zz, y, h)
            )
            self.lo = sems.msg(theirs, rows(z, y), y=yp)
            zs = [zk[0], zk[3], zk[1], zk[2]]
            def front(zz, yy):
                return buf.at[pl.ds(_mo((zz * 4 + yy) * ROWS, 16), ROWS - tail)]

            def back(zz, yy, h):
                at = (zz * 4 + yy) * ROWS + ROWS - tail + h * (tail // 2)
                return buf.at[pl.ds(_mo(at, 16), tail // 2)]

            self.u = [sems.msg(mine, rows(z, y), y=yh)]
            self.u += [sems.msg(front(zz, y), front(zz, y), y=yh) for zz in zs[1:]]
            if tail:
                self.b3 = Bcast(sems, "z", z, lambda h: back(z, yh, h), lambda zz, h: back(zz, yh, h))
            self.u4 = sems.msg(rows(z, yp), rows(z, yp), y=yh)
            self.b1 = Bcast(sems, "z", z, lambda h: rows(z, yp, h), lambda zz, h: rows(zz, yp, h))
            self.b2 = Bcast(sems, "z", z, lambda h: rows(z, yq, h), lambda zz, h: rows(zz, yq, h))
            self.mine, self.buf, self.tail = mine, buf, tail

        def keep(self):
            self.buf[pl.ds(_mo((z * 4 + y) * ROWS, 16), ROWS), :] = self.mine[...]

        def n1(self):
            self.b0.m2.wait_recv()
            self.u[1].start()

        def n2(self):
            self.b0.m3.wait_recv()
            self.u[2].start()

        def far(self):
            self.b0.far()
            self.u[3].start()

        def arrived(self):
            self.b1.near()
            self.b1.far()
            self.b2.near()
            self.b2.far()
            if self.tail:
                self.b3.near()
                self.b3.far()
            for m in self.u[1 if self.tail else 0 :]:
                m.wait_recv()

    class Acts:
        def __init__(self, own, buf, kind):
            def slot(xx, h=None):
                lanes = pl.ds(_mo((xx * 2 + c) * FEAT, 128), FEAT)
                if h is None:
                    return buf.at[pl.ds(kind * TOK, TOK), lanes]
                return buf.at[pl.ds(kind * TOK + h * 256, 256), lanes]

            half = (lambda h: own.at[pl.ds(h * 256, 256)]) if kind == 0 else (lambda h: slot(x, h))
            self.b = Bcast(sems, "x", x, half, slot)
            xs = [xk[0], xk[3], xk[1], xk[2]]
            self.d = [
                sems.msg(own if (k == 0 and kind == 0) else slot(xx), slot(xx), c=sib)
                for k, xx in enumerate(xs)
            ]
            if kind == 0:
                lanes = pl.ds(_mo(tp * FEAT, 128), FEAT)
                self.lo = [
                    sems.msg(own.at[pl.ds(h * 256, 256)], buf.at[pl.ds(TOK + h * 256, 256), lanes], y=yp) for h in (0, 1)
                ]

        def n1(self):
            self.b.m2.wait_recv()
            self.d[1].start()

        def n2(self):
            self.b.m3.wait_recv()
            self.d[2].start()

        def far(self):
            self.b.far()
            self.d[3].start()

        def arrived(self):
            for m in self.d:
                m.wait_recv()

    class Reduce:
        def __init__(self, src, got, hb, hq, lin, tail=0, tgot=None, tin=None):
            def rows(zz, yy, h=None):
                if h is None:
                    return src.at[pl.ds(_mo((zz * 4 + yy) * ROWS, 16), ROWS)]
                return src.at[pl.ds(_mo((zz * 4 + yy) * ROWS + h * 96, 16), 96)]

            self.rows, self.hb, self.hq, self.lin = rows, hb, hq, lin
            self.zq = Scatter(sems, "z", z, lambda zz, h: rows(zz, yq, h), got.at[0], 96, 48)
            self.zp = Scatter(sems, "z", z, lambda zz, h: rows(zz, yp, h), got.at[1], 96, 48)
            part = (ROWS - tail) // 2
            self.part = part

            def front(zz, yy, h):
                return src.at[pl.ds(_mo((zz * 4 + yy) * ROWS + h * part, 16), part)]

            def back(zz, yy, h):
                at = (zz * 4 + yy) * ROWS + ROWS - tail + h * (tail // 2)
                return src.at[pl.ds(_mo(at, 16), tail // 2)]

            self.zo = Scatter(
                sems, "z", z, lambda zz, h: front(zz, y, h), got.at[2, :, pl.ds(0, part)], part, 16 if tail else 48
            )
            if tail:
                self.zh = Scatter(sems, "z", z, lambda zz, h: back(zz, yh, h), tgot.at[0], tail // 2, 16)
                self.zb = Scatter(sems, "z", z, lambda zz, h: back(zz, y, h), tgot.at[1], tail // 2, 16)
                whole = src.at[pl.ds(_mo((z * 4 + yh) * ROWS + ROWS - tail, 16), tail)]
                self.x = sems.msg(whole, tin, y=yh)
                self.tin, self.tail = tin, tail
            keep = pl.ds(0, ROWS - tail)
            self.v = [sems.msg(rows(zk[k], yh).at[keep], hb.at[k, keep], y=yh) for k in range(4)]
            half = [pl.ds(0, 96), pl.ds(96, 96)]
            self.w = [sems.msg(rows(z, yq, h), hq.at[half[h]], y=yh) for h in (0, 1)]
            self.l = [sems.msg(rows(z, yp, h), lin.at[half[h]], y=yp) for h in (0, 1)]

        def merge_hi(self, k):
            self.v[k].wait_recv()
            add_to(self.rows(zk[k], y), self.hb.at[k], 2 * self.part, 32 if self.part % 48 else 48)

        def q(self, h):
            own = self.rows(z, yq)

            def put(h, i, n, total):
                own[pl.ds(_mo(h * 96 + i, 16), n), :] = total.astype(BF)

            self.zq.last(h, put)
            self.w[h].start()

        def p(self, h):
            self.w[h].wait_recv()
            own = self.rows(z, yp)

            def put(h, i, n, total):
                r = pl.ds(_mo(h * 96 + i, 16), n)
                own[r, :] = (total + self.hq[r, :].astype(F32)).astype(BF)

            self.zp.last(h, put)
            self.l[h].start()

        def o(self, h, outs):
            def put(h, i, n, total):
                write(outs, hs, h * self.part + i, n, total)

            self.zo.last(h, put)

        def cross(self):
            own = self.rows(z, yh)

            def put(h, i, n, total):
                own[pl.ds(_mo(ROWS - self.tail + h * (self.tail // 2) + i, 16), n), :] = total.astype(BF)

            self.zh.last(0, put)
            self.zh.last(1, put)
            self.x.start()

        def ob(self, outs):
            self.x.wait_recv()

            def put(h, i, n, total):
                at = h * (self.tail // 2) + i
                write(outs, hs, ROWS - self.tail + at, n, total + self.tin[pl.ds(_mo(at, 16), n), :].astype(F32))

            self.zb.last(0, put)
            self.zb.last(1, put)

        def t(self, h, outs):
            self.l[h].wait_recv()

            @pl.loop(0, 2)
            def _(i):
                at = _mo(h * 96 + i * 48, 16)
                write(outs, 1 - hs, at, 48, self.lin[pl.ds(at, 48), :].astype(F32))

    def write(outs, half, row, n, value):
        r = pl.ds(_mo(row, 16), n)
        for j, out in enumerate(outs):
            part = value[:, j * HALF : (j + 1) * HALF]
            rest = out.shape[1] - HALF

            @pl.when(half == 0)
            def _():
                out[r, :HALF] = part

            @pl.when(half == 1)
            def _():
                out[r, HALF:] = part[:, :rest]

    gd = Gather(wdm, wdt, Wd)
    gw = Gather(wgm, wgt, Wg, 32)
    go, gp = Acts(gpo, GP, 0), Acts(None, GP, 1)
    xo, xp = Acts(xin, X, 0), Acts(None, X, 1)
    plo = sems.msg(pt, PRE.at[:, pl.ds(TOK, TOK)], y=yp)
    stats = [sems.msg(st.at[0], st.at[k], **tps[k - 1]) for k in range(1, 8)]
    sd = Reduce(Dd, dgot, dhb, dhq, dlin)
    sw = Reduce(Dg, ggot, ghb, ghq, glin, 32, tgot, tin)
    e = [sems.msg(CS.at[k], E.at[k], c=sib) for k in range(4)]
    xs = Scatter(sems, "x", x, lambda xx, h: MC.at[lax.rem(xx - x + 4, 4), pl.ds(h * TOK, TOK)], xgot, TOK, 64)
    xl = sems.msg(MC.at[0, pl.ds(TOK, TOK)], xlin, y=yp)
    sz_m = [sems.msg(small, sz.at[k - 1], z=zk[k]) for k in (1, 2, 3)]
    sy_m = [sems.msg(sy.at[3], sy.at[k], y=yy) for k, yy in enumerate((yh, yp, yq))]

    def grad_act(kind):
        @pl.loop(0, 2)
        def _(i):
            r = pl.ds(_mo(kind * TOK + i * 256, 256), 256)
            GA[r, :] = mm(GP[r, :], Wd[...], 1, 0)

    def middle(kind, lo, hi):
        row = lax.broadcasted_iota(jnp.int32, (SEQ, 128), 0)

        def prev(v):
            return jnp.where(row == 0, 0.0, pltpu.roll(v, 1, 0))

        def succ(v):
            return jnp.where(row == SEQ - 1, 0.0, pltpu.roll(v, SEQ - 1, 0))

        @pl.loop(lo, hi)
        def _(i):
            r = pl.ds(_mo(kind * TOK + (i // 3) * SEQ, SEQ), SEQ)
            at = lax.rem(i, 3) * 128
            lanes, lanes2 = pl.ds(_mo(at, 128), 128), pl.ds(_mo(HALF + at, 128), 128)
            gate = PRE[lanes, r].astype(F32).T
            value = PRE[lanes2, r].astype(F32).T
            t0, t1, t2 = (tap[k : k + 1, lanes] for k in range(3))
            before, after = prev(gate), succ(gate)
            mixed = t0 * before + t1 * gate + t2 * after
            sig = jax.nn.sigmoid(mixed)
            active = mixed * sig
            ga = GA[r, lanes]
            hid[r, lanes] = (active * value).astype(BF)
            G[r, lanes2] = (ga * active).astype(BF)
            gm = ga * value * sig * (1.0 + mixed * (1.0 - sig))
            G[r, lanes] = (t1 * gm + t0 * succ(gm) + t2 * prev(gm)).astype(BF)
            for k, v in enumerate((before, gate, after)):
                tacc[k, :, lanes] += jnp.sum((gm * v).reshape(SEQ // 8, 8, 128), axis=0)

    def block(dst, left, right, zz, yy):
        at = _mo((zz * 2 + yy // 2) * FEAT, 128)
        dst[pl.ds(at, FEAT), :] = mm(left[:, pl.ds(at, FEAT)], right[...], 0, 0).astype(BF)

    def blocks(dst, left, right, yy, first):
        @pl.loop(0, 2)
        def _(k):
            zz = lax.rem(z + 2 - k + 4, 4) if first else lax.rem(z + 3 + k, 4)
            block(dst, left, right, zz, yy)

    def contrib(dst, cc, first, other=None):
        @pl.loop(0, 2)
        def _(i):
            k = 2 - i if first else lax.rem(3 + i, 4)
            at = _mo((lax.rem(x + k, 4) * 2 + cc) * FEAT, 128)
            term = mm(G[...], Wg[pl.ds(at, FEAT), :], 1, 1)
            if other is not None:
                term = term + other[k].astype(F32)
            dst[k] = term.astype(BF)

    pl.semaphore_wait(barrier, 13)
    for m in stats:
        m.start()
    gd.b0.m3.start()
    gd.lo.start()
    xo.d[0].start()
    xo.b.m0.start()
    gd.b0.m2.start()
    gd.u[0].start()
    xo.b.m1.start()
    gd.b0.m1.start()
    gd.b0.m0.start()
    own_lanes = pl.ds(_mo(tp * FEAT, 128), FEAT)
    X[0:TOK, own_lanes] = xin[...]
    gd.keep()
    split(taps, tap, None)
    tacc[...] = jnp.zeros_like(tacc)
    for m in loads[2:4]:
        m.wait()
    split(gatew, wgm.at[:, 0:HALF], wgt.at[:, 0:HALF])
    split(valuew, wgm.at[:, HALF : 2 * HALF], wgt.at[:, HALF : 2 * HALF])
    gw.keep()
    gw.b0.m1.start()
    gw.b0.m2.start()
    gw.b0.m3.start()
    gw.u[0].start()
    gw.b0.m0.start()
    for m in stats:
        m.wait_recv()
    tot = st[0]
    for k in range(1, 8):
        tot = tot + st[k]
    inverse = lax.rsqrt(tot[0:4] / D + EPSILON)
    coef = inverse * inverse * (tot[4:8] / D)

    def column(v):
        v = jnp.concatenate([jnp.broadcast_to(v[i : i + 1], (128, 128)).T for i in range(4)], axis=0)
        return jnp.concatenate([v, v, v], axis=1)

    inv = column(inverse)
    pf = pre[...].astype(F32)
    cf = cot[...].astype(F32)
    scaled = gain[...][None, :] * cf
    g = (inv * (scaled - pf * column(coef))).astype(BF)
    gpo[...] = g
    GP[0:TOK, own_lanes] = g
    small[...] = jnp.broadcast_to(jnp.sum(cf * pf * inv, axis=0, keepdims=True), (8, FEAT))
    go.lo[0].start()
    go.b.m3.start()
    go.lo[1].start()
    go.b.m1.start()
    go.b.m0.start()
    go.b.m2.start()
    go.d[0].start()
    gd.lo.wait_recv()
    gd.b1.m1.start()
    gd.b1.m3.start()
    gd.b1.m0.start()
    gd.b1.m2.start()
    gd.u4.start()
    gd.b0.f0()
    gw.lo.start()
    for m in loads[4:]:
        m.wait()
    split_rows(saved.at[0], PRE.at[0:HALF, 0:TOK], pt.at[0:HALF])
    split_rows(saved.at[1], PRE.at[HALF : 2 * HALF, 0:TOK], pt.at[HALF : 2 * HALF])

    gd.b0.f1()
    gd.n2()
    gd.n1()
    plo.start()
    xo.lo[0].start()
    xo.lo[1].start()
    gd.b1.f0()
    go.lo[0].wait_recv()
    gp.b.m3.start()
    gp.b.m0.start()
    gw.b0.f1()
    go.lo[1].wait_recv()
    gp.b.m2.start()
    gp.b.m1.start()
    gp.d[0].start()
    go.b.f1()
    go.n2()
    gd.u4.wait_recv()
    gd.b2.m3.start()
    gd.b2.m2.start()
    gd.b2.m1.start()
    gd.b2.m0.start()
    gw.u[0].wait_recv()
    gw.b3.m3.start()
    gw.b3.m1.start()
    gw.b3.m0.start()
    gw.b3.m2.start()
    gd.far()
    go.b.f0()
    gw.b0.f0()
    gd.b1.f1()
    gw.lo.wait_recv()
    gw.b1.m0.start()
    gw.b1.m1.start()
    gw.b1.m2.start()
    gw.u4.start()
    gw.b1.m3.start()
    gd.b2.f1()
    gw.b3.f1()
    gw.n2()
    go.n1()
    gp.b.f0()
    gp.b.f1()
    xo.b.m3.start()
    xo.b.m2.start()
    xo.b.f1()
    gw.n1()
    gd.b2.f0()
    gw.b3.f0()
    go.far()
    gw.u4.wait_recv()
    gw.b2.m1.start()
    gw.b2.m0.start()
    gw.b2.m2.start()
    gw.b2.m3.start()
    gp.n1()
    go.arrived()
    xo.b.f0()
    gw.b1.f0()
    gp.n2()
    gd.arrived()
    gp.far()
    gw.b1.f1()
    grad_act(0)
    middle(0, 0, 6)
    gp.arrived()
    gw.b2.f1()
    gw.b2.f0()
    gw.far()
    grad_act(1)
    xo.n1()
    middle(0, 6, 12)
    plo.wait_recv()
    middle(1, 0, 6)
    xo.lo[0].wait_recv()
    xp.b.m3.start()
    xp.b.m0.start()
    xo.n2()
    middle(1, 6, 12)
    xo.far()
    blocks(Dd, GP, hid, yh, True)
    sd.zq.m2.start()
    sd.zq.m1.start()
    sd.v[2].start()
    sd.v[1].start()
    sd.zq.m0.start()
    blocks(Dd, GP, hid, yh, False)
    sd.v[3].start()
    sd.zq.m3.start()
    sd.v[0].start()
    gw.arrived()
    xo.lo[1].wait_recv()
    xp.b.m2.start()
    xp.d[0].start()
    xp.b.m1.start()
    contrib(CS, sib, True)
    e[1].start()
    e[2].start()
    for k in range(3):
        small[k : k + 1, :] = jnp.sum(tacc[k], axis=0, keepdims=True)
    for m in sz_m:
        m.start()
    xp.b.f0()
    blocks(Dd, GP, hid, y, True)
    sd.zp.m0.start()
    sd.zp.m2.start()
    sd.zp.m1.start()
    contrib(CS, sib, False)
    e[3].start()
    e[0].start()
    sd.merge_hi(2)
    sd.zo.m0.start()
    sd.zo.m1.start()
    xp.b.f1()
    blocks(Dd, GP, hid, y, False)
    sd.zp.m3.start()
    xp.n1()
    sd.merge_hi(1)
    sd.zo.m2.start()
    sd.zq.g1()
    e[2].wait_recv()
    e[1].wait_recv()
    contrib(MC, c, True, E)
    xs.m0.start()
    xs.m2.start()
    xs.m1.start()
    sd.zp.g1()
    xp.n2()
    sd.zq.g0()
    sd.merge_hi(3)
    sd.zo.m3.start()
    for m in sz_m:
        m.wait_recv()
    sy[3] = small[...] + sz[0] + sz[1] + sz[2]
    for m in sy_m:
        m.start()
    xp.far()
    e[3].wait_recv()
    e[0].wait_recv()
    contrib(MC, c, False, E)
    xs.m3.start()
    xo.arrived()
    sd.q(0)
    sd.q(1)
    sd.zp.g0()
    xp.arrived()
    blocks(Dg, X, G, yh, True)
    sw.zq.m2.start()
    sw.zh.m2.start()
    sw.v[1].start()
    sw.v[2].start()
    sw.zq.m1.start()
    sw.zh.m1.start()
    sw.zh.m0.start()
    sw.zq.m0.start()
    blocks(Dg, X, G, yh, False)
    sw.v[0].start()
    sw.v[3].start()
    sw.zh.m3.start()
    sw.zq.m3.start()
    blocks(Dg, X, G, y, True)
    sw.zp.m0.start()
    sw.zp.m1.start()
    sw.zb.m0.start()
    sw.zp.m2.start()
    sw.zb.m2.start()
    sw.zb.m1.start()
    xs.g0()
    xs.g1()
    blocks(Dg, X, G, y, False)
    sw.zp.m3.start()
    sw.zb.m3.start()
    sw.zq.g1()
    sd.p(0)
    for m in sy_m:
        m.wait_recv()
    rest = gt_out.shape[1] - HALF
    mine_sum = sy[3] + sy[0]
    their_sum = sy[1] + sy[2]

    @pl.when(hs == 0)
    def _():
        gt_out[:, :HALF] = mine_sum[0:3]
        gt_out[:, HALF:] = their_sum[0:3, :rest]

    @pl.when(hs == 1)
    def _():
        gt_out[:, :HALF] = their_sum[0:3]
        gt_out[:, HALF:] = mine_sum[0:3, :rest]

    gn_out[...] = (mine_sum[3:4] + their_sum[3:4])[0]
    stores[4].start()
    stores[5].start()
    sd.zo.g0()
    sw.zh.g0()
    sw.zq.g0()
    sd.zo.g1()
    sw.zp.g1()
    sd.p(1)
    def put1(h, i, n, total):
        MC[0, pl.ds(_mo(TOK + i, 16), n), :] = total.astype(BF)

    xs.last(1, put1)
    xl.start()
    sd.merge_hi(0)

    sw.q(1)
    def put0(h, i, n, total):
        GA[pl.ds(_mo(i, 16), n), :] = total

    xs.last(0, put0)
    sw.merge_hi(2)
    sw.zo.m0.start()
    sw.zo.m1.start()
    sw.q(0)
    sw.zp.g0()
    sw.merge_hi(1)
    sw.zo.m2.start()
    sw.zh.g1()
    sw.merge_hi(3)
    sw.zo.m3.start()
    sw.p(1)
    sw.zb.g1()
    sd.t(1, (gd_out,))
    sw.zo.g1()
    sw.zo.g0()
    sw.p(0)
    sd.t(0, (gd_out,))
    sw.cross()
    sw.merge_hi(0)

    sw.zb.g0()
    sd.o(1, (gd_out,))
    sw.o(0, (gg_out, gv_out))
    sw.t(1, (gg_out, gv_out))
    sw.o(1, (gg_out, gv_out))
    sw.ob((gg_out, gv_out))
    xl.wait_recv()

    @pl.loop(0, 8)
    def _(i):
        r = pl.ds(_mo(i * 64, 16), 64)
        gi[r, :] = (GA[r, :] + xlin[r, :].astype(F32)).astype(BF)

    stores[0].start()
    sd.o(0, (gd_out,))
    stores[3].start()
    sw.t(0, (gg_out, gv_out))
    stores[1].start()
    stores[2].start()
    for m in stores:
        m.wait()
    sems.drain()


N = 7 + 2 * 24 + 4 * 10 + 2 + 1 + 2 + 2 * 26 + 4 + 6 + 1 + 6 + 19
VM = pl.BlockSpec(memory_space=pltpu.VMEM)
ANY = pl.BlockSpec(memory_space=pl.ANY)


def hand_on(*refs):
    src, dst, here = refs[:6], refs[6:12], refs[12:18]
    took = [pltpu.make_async_copy(a, b, refs[18].at[k]) for k, (a, b) in enumerate(zip(src, here))]
    gave = [pltpu.make_async_copy(a, b, refs[19].at[k]) for k, (a, b) in enumerate(zip(here, dst))]
    for m in took:
        m.start()
    for k in (1, 2, 3, 0, 4, 5):
        took[k].wait()
        gave[k].start()
    for m in gave:
        m.wait()


def on_device(
    inputs, cotangent, pre_norm, gate_pre, value_pre, gate_weight, value_weight, down_weight, conv_taps, norm_gain
):
    width = gate_pre.shape[1]

    def vm(*shape, dtype=BF):
        return pltpu.VMEM(shape, dtype)

    def wscratch(n):
        return [vm(3, 6, 96, n), vm(4, ROWS, n), vm(ROWS, n), vm(ROWS, n)]

    two = 2 * TOK
    outs = pl.pallas_call(
        kernel,
        out_shape=(
            jax.ShapeDtypeStruct((TOK, FEAT), BF),
            jax.ShapeDtypeStruct((ROWS, width), F32),
            jax.ShapeDtypeStruct((ROWS, width), F32),
            jax.ShapeDtypeStruct((ROWS, width), F32),
            jax.ShapeDtypeStruct((3, width), F32),
            jax.ShapeDtypeStruct((FEAT,), F32),
        ),
        in_specs=[VM] * 3 + [ANY] * 6 + [VM],
        out_specs=(ANY,) * 6,
        scratch_shapes=[
            vm(two, D), vm(two, D), vm(D, HALF), vm(D, 2 * HALF), vm(2 * HALF, two),
            vm(8, 8, 128, dtype=F32), vm(TOK, FEAT),
            vm(ROWS, HALF), vm(ROWS, HALF), vm(ROWS, 2 * HALF), vm(ROWS, 2 * HALF),
            vm(2 * HALF, TOK), vm(3, HALF, dtype=F32), vm(2, width, TOK), vm(2, 6, 16, 2 * HALF), vm(32, 2 * HALF),
            vm(TOK, FEAT), vm(ROWS, width), vm(ROWS, width), vm(ROWS, width),
            vm(TOK, FEAT), vm(ROWS, width, dtype=F32), vm(ROWS, width, dtype=F32), vm(ROWS, width, dtype=F32),
            vm(3, width, dtype=F32), vm(FEAT, dtype=F32),
            vm(two, HALF, dtype=F32), vm(two, HALF), vm(two, 2 * HALF), vm(3, 8, HALF, dtype=F32),
            vm(D, HALF), vm(D, 2 * HALF),
            vm(4, two, FEAT), vm(4, two, FEAT), vm(4, two, FEAT), vm(6, TOK, FEAT), vm(TOK, FEAT),
        ]
        + wscratch(HALF)
        + wscratch(2 * HALF)
        + [
            vm(8, FEAT, dtype=F32), vm(3, 8, FEAT, dtype=F32), vm(4, 8, FEAT, dtype=F32),
            pltpu.SemaphoreType.DMA((N,)),
            pltpu.SemaphoreType.DMA((N,)),
            pltpu.SemaphoreType.DMA((12,)),
        ],
        compiler_params=pltpu.CompilerParams(
            collective_id=0, has_side_effects=True, vmem_limit_bytes=67043328
        ),
        name="layer",
    )(
        pre_norm, cotangent, norm_gain, inputs, down_weight.T,
        gate_weight, value_weight, gate_pre.T, value_pre.T, conv_taps,
    )
    outs = pl.pallas_call(
        hand_on,
        out_shape=tuple(jax.ShapeDtypeStruct(a.shape, a.dtype) for a in outs),
        in_specs=[ANY] * 6,
        out_specs=(ANY,) * 6,
        scratch_shapes=[pltpu.VMEM(a.shape, a.dtype) for a in outs]
        + [pltpu.SemaphoreType.DMA((6,)), pltpu.SemaphoreType.DMA((6,))],
        name="hand_on",
    )(*outs)
    gi, gg, gv, gd, gt, gn = outs
    return (gi, gg, gv, gd.T, gt, gn)


def solution(mesh):
    split = Mesh(mesh.devices.reshape(4, 4, 4, 2), ("z", "y", "x", "c"))
    fs, tp = ("z", "y"), ("x", "c")
    both, across = P(fs, tp), P(tp, fs)
    in_specs = (both, both, both, both, both, both, both, across, P(None, tp), P(tp))
    out_specs = (both, both, both, across, P(None, tp), P(tp))
    return jax.shard_map(on_device, mesh=split, in_specs=in_specs, out_specs=out_specs, check_vma=False)
```

```python
import jax
import jax.numpy as jnp
from jax import lax
from jax.experimental import pallas as pl
from jax.experimental.pallas import tpu as pltpu
from jax.sharding import Mesh
from jax.sharding import PartitionSpec as P

D = 3072
SEQ = 128
EPSILON = 1e-06
HALF = 384
ROWS = 192
TOK = 512
FEAT = 384
BF = jnp.bfloat16
F32 = jnp.float32
MESH = pl.DeviceIdType.MESH


def _mo(v, m):
    return pl.multiple_of(v, m)


class Sems:
    def __init__(self, send, recv, units):
        self.send, self.recv, self.units = send, recv, units
        self.n, self.k, self.open, self.groups = 0, 0, {}, []

    def _send(self, src):
        key, rows = src.shape[1:] if len(src.shape) == 2 else None, src.shape[0]
        if src.dtype == F32:
            key, rows = src.shape, 1
        if key not in self.units:
            self.groups.append([src, None])
            return len(self.groups) - 1
        ref, cap = self.units[key]
        at = self.open.get(key)
        if at is None or self.groups[at][1] + rows > cap:
            at = self.open[key] = len(self.groups)
            self.groups.append([ref, 0])
        self.groups[at][1] += rows
        return at

    def joint(self):
        self.n += 1
        return self.n - 1

    def msg(self, src, dst, share=None, **dev):
        return pltpu.make_async_remote_copy(
            src_ref=src,
            dst_ref=dst,
            send_sem=self.send.at[self._send(src)],
            recv_sem=self.recv.at[self.joint() if share is None else share],
            device_id=dev,
            device_id_type=MESH,
        )

    def take(self, share, ref):
        pltpu.make_async_copy(ref, ref, self.recv.at[share]).wait()

    def drain(self):
        assert len(self.groups) <= NS and self.n <= N
        for k, (ref, rows) in enumerate(self.groups):
            if rows is not None:
                ref = ref.at[pl.ds(0, rows)]
            pltpu.make_async_copy(ref, ref, self.send.at[k]).wait()


class Bcast:
    def __init__(self, sems, axis, me, own, slot):
        up, down = lax.rem(me + 1, 4), lax.rem(me + 3, 4)
        to_up, to_down = {axis: up}, {axis: down}
        self.m0 = sems.msg(own(0), slot(me, 0), **to_up)
        self.m1 = sems.msg(own(1), slot(me, 1), **to_down)
        self.m2 = sems.msg(own(1), slot(me, 1), **to_up)
        self.m3 = sems.msg(own(0), slot(me, 0), **to_down)
        self.m4 = sems.msg(slot(down, 0), slot(down, 0), **to_up)
        self.m5 = sems.msg(slot(up, 1), slot(up, 1), **to_down)

    def f0(self):
        self.m0.wait_recv()
        self.m4.start()

    def f1(self):
        self.m1.wait_recv()
        self.m5.start()

    def near(self):
        self.m2.wait_recv()
        self.m3.wait_recv()

    def far(self):
        self.m4.wait_recv()
        self.m5.wait_recv()


class Scatter:
    def __init__(self, sems, axis, me, chunk, got, rows, step):
        up, down = lax.rem(me + 1, 4), lax.rem(me + 3, 4)
        far = lax.rem(me + 2, 4)
        to_up, to_down = {axis: up}, {axis: down}
        self.me, self.up, self.down = me, up, down
        self.chunk, self.got, self.rows, self.step = chunk, got, rows, step
        self.m0 = sems.msg(chunk(far, 0), got.at[0], **to_up)
        self.m1 = sems.msg(chunk(far, 1), got.at[1], **to_down)
        self.m2 = sems.msg(chunk(up, 1), got.at[2], **to_up)
        self.m3 = sems.msg(chunk(down, 0), got.at[3], **to_down)
        self.m4 = sems.msg(chunk(up, 0), got.at[4], **to_up)
        self.m5 = sems.msg(chunk(down, 1), got.at[5], **to_down)

    def g0(self):
        self.m0.wait_recv()
        add_to(self.chunk(self.up, 0), self.got.at[0], self.rows, self.step)
        self.m4.start()

    def g1(self):
        self.m1.wait_recv()
        add_to(self.chunk(self.down, 1), self.got.at[1], self.rows, self.step)
        self.m5.start()

    def last(self, h, put):
        a, b = ((3, 4), (2, 5))[h]
        (self.m3, self.m2)[h].wait_recv()
        (self.m4, self.m5)[h].wait_recv()
        n = self.step
        own = self.chunk(self.me, h)

        @pl.loop(0, self.rows // n)
        def _(i):
            r = pl.ds(_mo(i * n, 16), n)
            put(h, i * n, n, own[r, :].astype(F32) + self.got[a, r, :].astype(F32) + self.got[b, r, :].astype(F32))


def add_to(dst, src, rows, step):
    @pl.loop(0, rows // step)
    def _(i):
        r = pl.ds(_mo(i * step, 16), step)
        dst[r, :] = (dst[r, :].astype(F32) + src[r, :].astype(F32)).astype(BF)


def mm(a, b, ca, cb):
    return lax.dot_general(a, b, (((ca,), (cb,)), ((), ())), preferred_element_type=F32)


def kernel(
    pre, cot, gain, xin_hbm, down_hbm, gatew_hbm, valuew_hbm, gatep, valuep, taps,
    *refs,
):
    results, scratch = refs[:6], refs[6:]
    (
        GP, X, Wd, Wg, PRE, st, gpo, wdm,
        wdt, wgm, wgt, pt, tap, saved, tgot, tin, xin, down,
        gatew, valuew, gi, gg_out, gv_out, gd_out, gt_out, gn_out,
        GA, hid, G, tacc, Dd, Dg, CS, MC,
        E, xgot, xlin, dgot, dhb, dhq, dlin, ggot,
        ghb, ghq, glin, small, sz, sy, ss, rs,
        ls,
    ) = scratch
    z, y = lax.axis_index("z"), lax.axis_index("y")
    x, c = lax.axis_index("x"), lax.axis_index("c")
    yp = y + 1 - 2 * lax.rem(y, 2)
    yh = 3 - y
    yq = yh + 1 - 2 * lax.rem(yh, 2)
    hs = lax.rem((y + 1) // 2, 2)
    sib = 1 - c
    tp = x * 2 + c
    zk = [lax.rem(z + k, 4) for k in range(4)]
    xk = [lax.rem(x + k, 4) for k in range(4)]
    units = {(HALF,): (Dd, D), (2 * HALF,): (Dg, D), (8, 128): (st, 8), (8, FEAT): (sz, 3)}
    sems = Sems(ss, rs, units)
    hbm = (down_hbm, xin_hbm, gatew_hbm, valuew_hbm, gatep, valuep)
    here = (down, xin, gatew, valuew, saved.at[0], saved.at[1])
    loads = [pltpu.make_async_copy(a, b, ls.at[k]) for k, (a, b) in enumerate(zip(hbm, here))]
    for m in loads:
        m.start()
    found = (gi, gg_out, gv_out, gd_out, gt_out, gn_out)
    stores = [pltpu.make_async_copy(a, b, ls.at[6 + k]) for k, (a, b) in enumerate(zip(found, results))]

    barrier = pltpu.get_barrier_semaphore()
    peers = [{"z": zk[1]}, {"z": zk[2]}, {"z": zk[3]}, {"y": yp}, {"y": yh}, {"y": yq}]
    tps = []
    for k in range(1, 8):
        t = lax.rem(tp + k, 8)
        tps.append({"x": t // 2, "c": lax.rem(t, 2)})
    for dev in peers + tps:
        pl.semaphore_signal(barrier, inc=1, device_id=dev, device_id_type=MESH)

    def lane_sums(v):
        v = v[:, :128] + v[:, 128:256] + v[:, 256:384]
        return jnp.sum(v.T, axis=0, keepdims=True)

    pf = pre[...].astype(F32)
    cf = cot[...].astype(F32)
    scaled = gain[...][None, :] * cf
    for j, v in enumerate((lane_sums(pf * pf), lane_sums(pf * scaled))):
        for i in range(4):
            st[0, j * 4 + i : j * 4 + i + 1, :] = v[:, i * 128 : (i + 1) * 128]

    def split(src, mine, theirs):
        n = src.shape[0]
        rest = src.shape[1] - HALF
        fill = jnp.zeros((n, HALF - rest), src.dtype)

        @pl.when(hs == 0)
        def _():
            mine[...] = src[:, :HALF]
            if theirs is not None:
                theirs[:, :rest] = src[:, HALF:]
                theirs[:, rest:] = fill

        @pl.when(hs == 1)
        def _():
            mine[:, :rest] = src[:, HALF:]
            mine[:, rest:] = fill
            if theirs is not None:
                theirs[...] = src[:, :HALF]

    loads[0].wait()
    split(down, wdm, wdt)
    loads[1].wait()

    def split_rows(src, mine, theirs):
        rest = src.shape[0] - HALF
        fill = jnp.zeros((HALF - rest, src.shape[1]), src.dtype)

        @pl.when(hs == 0)
        def _():
            mine[...] = src[:HALF]
            theirs[:rest] = src[HALF:]
            theirs[rest:] = fill

        @pl.when(hs == 1)
        def _():
            mine[:rest] = src[HALF:]
            mine[rest:] = fill
            theirs[...] = src[:HALF]

    class Gather:
        def __init__(self, mine, theirs, buf, tail=0):
            def rows(zz, yy, h=None):
                if h is None:
                    return buf.at[pl.ds(_mo((zz * 4 + yy) * ROWS, 16), ROWS)]
                return buf.at[pl.ds(_mo((zz * 4 + yy) * ROWS + h * 96, 16), 96)]

            self.b0 = Bcast(
                sems, "z", z, lambda h: mine.at[pl.ds(h * 96, 96)], lambda zz, h: rows(zz, y, h)
            )
            self.lo = sems.msg(theirs, rows(z, y), y=yp)
            zs = [zk[0], zk[3], zk[1], zk[2]]
            def front(zz, yy):
                return buf.at[pl.ds(_mo((zz * 4 + yy) * ROWS, 16), ROWS - tail)]

            def back(zz, yy, h):
                at = (zz * 4 + yy) * ROWS + ROWS - tail + h * (tail // 2)
                return buf.at[pl.ds(_mo(at, 16), tail // 2)]

            self.u = [sems.msg(mine, rows(z, y), y=yh)]
            self.u += [sems.msg(front(zz, y), front(zz, y), y=yh) for zz in zs[1:]]
            if tail:
                self.b3 = Bcast(sems, "z", z, lambda h: back(z, yh, h), lambda zz, h: back(zz, yh, h))
            self.u4 = sems.msg(rows(z, yp), rows(z, yp), y=yh)
            self.b1 = Bcast(sems, "z", z, lambda h: rows(z, yp, h), lambda zz, h: rows(zz, yp, h))
            self.b2 = Bcast(sems, "z", z, lambda h: rows(z, yq, h), lambda zz, h: rows(zz, yq, h))
            self.mine, self.buf, self.tail = mine, buf, tail

        def keep(self):
            self.buf[pl.ds(_mo((z * 4 + y) * ROWS, 16), ROWS), :] = self.mine[...]

        def n1(self):
            self.b0.m2.wait_recv()
            self.u[1].start()

        def n2(self):
            self.b0.m3.wait_recv()
            self.u[2].start()

        def far(self):
            self.b0.far()
            self.u[3].start()

        def arrived(self):
            self.b1.near()
            self.b1.far()
            self.b2.near()
            self.b2.far()
            if self.tail:
                self.b3.near()
                self.b3.far()
            for m in self.u[1 if self.tail else 0 :]:
                m.wait_recv()

    class Acts:
        def __init__(self, own, buf, kind):
            def slot(xx, h=None):
                lanes = pl.ds(_mo((xx * 2 + c) * FEAT, 128), FEAT)
                if h is None:
                    return buf.at[pl.ds(kind * TOK, TOK), lanes]
                return buf.at[pl.ds(kind * TOK + h * 256, 256), lanes]

            half = (lambda h: own.at[pl.ds(h * 256, 256)]) if kind == 0 else (lambda h: slot(x, h))
            self.b = Bcast(sems, "x", x, half, slot)
            xs = [xk[0], xk[3], xk[1], xk[2]]
            self.j = sems.joint()
            self.d = [
                sems.msg(own if (k == 0 and kind == 0) else slot(xx), slot(xx), self.j, c=sib)
                for k, xx in enumerate(xs)
            ]
            if kind == 0:
                lanes = pl.ds(_mo(tp * FEAT, 128), FEAT)
                self.lo = [
                    sems.msg(own.at[pl.ds(h * 256, 256)], buf.at[pl.ds(TOK + h * 256, 256), lanes], y=yp) for h in (0, 1)
                ]

        def n1(self):
            self.b.m2.wait_recv()
            self.d[1].start()

        def n2(self):
            self.b.m3.wait_recv()
            self.d[2].start()

        def far(self):
            self.b.far()
            self.d[3].start()

        def arrived(self):
            sems.take(self.j, Dd.at[pl.ds(0, 4 * TOK)])

    class Reduce:
        def __init__(self, src, got, hb, hq, lin, tail=0, tgot=None, tin=None):
            def rows(zz, yy, h=None):
                if h is None:
                    return src.at[pl.ds(_mo((zz * 4 + yy) * ROWS, 16), ROWS)]
                return src.at[pl.ds(_mo((zz * 4 + yy) * ROWS + h * 96, 16), 96)]

            self.rows, self.hb, self.hq, self.lin = rows, hb, hq, lin
            self.zq = Scatter(sems, "z", z, lambda zz, h: rows(zz, yq, h), got.at[0], 96, 48)
            self.zp = Scatter(sems, "z", z, lambda zz, h: rows(zz, yp, h), got.at[1], 96, 48)
            part = (ROWS - tail) // 2
            self.part = part

            def front(zz, yy, h):
                return src.at[pl.ds(_mo((zz * 4 + yy) * ROWS + h * part, 16), part)]

            def back(zz, yy, h):
                at = (zz * 4 + yy) * ROWS + ROWS - tail + h * (tail // 2)
                return src.at[pl.ds(_mo(at, 16), tail // 2)]

            self.zo = Scatter(
                sems, "z", z, lambda zz, h: front(zz, y, h), got.at[2, :, pl.ds(0, part)], part, 16 if tail else 48
            )
            if tail:
                self.zh = Scatter(sems, "z", z, lambda zz, h: back(zz, yh, h), tgot.at[0], tail // 2, 16)
                self.zb = Scatter(sems, "z", z, lambda zz, h: back(zz, y, h), tgot.at[1], tail // 2, 16)
                whole = src.at[pl.ds(_mo((z * 4 + yh) * ROWS + ROWS - tail, 16), tail)]
                self.x = sems.msg(whole, tin, y=yh)
                self.tin, self.tail = tin, tail
            keep = pl.ds(0, ROWS - tail)
            self.v = [sems.msg(rows(zk[k], yh).at[keep], hb.at[k, keep], y=yh) for k in range(4)]
            half = [pl.ds(0, 96), pl.ds(96, 96)]
            self.w = [sems.msg(rows(z, yq, h), hq.at[half[h]], y=yh) for h in (0, 1)]
            self.l = [sems.msg(rows(z, yp, h), lin.at[half[h]], y=yp) for h in (0, 1)]

        def merge_hi(self, k):
            self.v[k].wait_recv()
            add_to(self.rows(zk[k], y), self.hb.at[k], 2 * self.part, 32 if self.part % 48 else 48)

        def q(self, h):
            own = self.rows(z, yq)

            def put(h, i, n, total):
                own[pl.ds(_mo(h * 96 + i, 16), n), :] = total.astype(BF)

            self.zq.last(h, put)
            self.w[h].start()

        def p(self, h):
            self.w[h].wait_recv()
            own = self.rows(z, yp)

            def put(h, i, n, total):
                r = pl.ds(_mo(h * 96 + i, 16), n)
                own[r, :] = (total + self.hq[r, :].astype(F32)).astype(BF)

            self.zp.last(h, put)
            self.l[h].start()

        def o(self, h, outs):
            def put(h, i, n, total):
                write(outs, hs, h * self.part + i, n, total)

            self.zo.last(h, put)

        def cross(self):
            own = self.rows(z, yh)

            def put(h, i, n, total):
                own[pl.ds(_mo(ROWS - self.tail + h * (self.tail // 2) + i, 16), n), :] = total.astype(BF)

            self.zh.last(0, put)
            self.zh.last(1, put)
            self.x.start()

        def ob(self, outs):
            self.x.wait_recv()

            def put(h, i, n, total):
                at = h * (self.tail // 2) + i
                write(outs, hs, ROWS - self.tail + at, n, total + self.tin[pl.ds(_mo(at, 16), n), :].astype(F32))

            self.zb.last(0, put)
            self.zb.last(1, put)

        def t(self, h, outs):
            self.l[h].wait_recv()

            @pl.loop(0, 2)
            def _(i):
                at = _mo(h * 96 + i * 48, 16)
                write(outs, 1 - hs, at, 48, self.lin[pl.ds(at, 48), :].astype(F32))

    def write(outs, half, row, n, value):
        r = pl.ds(_mo(row, 16), n)
        for j, out in enumerate(outs):
            part = value[:, j * HALF : (j + 1) * HALF]
            rest = out.shape[1] - HALF

            @pl.when(half == 0)
            def _():
                out[r, :HALF] = part

            @pl.when(half == 1)
            def _():
                out[r, HALF:] = part[:, :rest]

    gd = Gather(wdm, wdt, Wd)
    gw = Gather(wgm, wgt, Wg, 32)
    go, gp = Acts(gpo, GP, 0), Acts(None, GP, 1)
    xo, xp = Acts(xin, X, 0), Acts(None, X, 1)
    plo = sems.msg(pt, PRE.at[:, pl.ds(TOK, TOK)], y=yp)
    stats_j, sz_j, sy_j = sems.joint(), sems.joint(), sems.joint()
    stats = [sems.msg(st.at[0], st.at[k], stats_j, **tps[k - 1]) for k in range(1, 8)]
    sd = Reduce(Dd, dgot, dhb, dhq, dlin)
    sw = Reduce(Dg, ggot, ghb, ghq, glin, 32, tgot, tin)
    e = [sems.msg(CS.at[k], E.at[k], c=sib) for k in range(4)]
    xs = Scatter(sems, "x", x, lambda xx, h: MC.at[lax.rem(xx - x + 4, 4), pl.ds(h * TOK, TOK)], xgot, TOK, 64)
    xl = sems.msg(MC.at[0, pl.ds(TOK, TOK)], xlin, y=yp)
    sz_m = [sems.msg(small, sz.at[k - 1], sz_j, z=zk[k]) for k in (1, 2, 3)]
    sy_m = [sems.msg(sy.at[3], sy.at[k], sy_j, y=yy) for k, yy in enumerate((yh, yp, yq))]

    def grad_act(kind):
        @pl.loop(0, 2)
        def _(i):
            r = pl.ds(_mo(kind * TOK + i * 256, 256), 256)
            GA[r, :] = mm(GP[r, :], Wd[...], 1, 0)

    def middle(kind, lo, hi):
        row = lax.broadcasted_iota(jnp.int32, (SEQ, 128), 0)

        def prev(v):
            return jnp.where(row == 0, 0.0, pltpu.roll(v, 1, 0))

        def succ(v):
            return jnp.where(row == SEQ - 1, 0.0, pltpu.roll(v, SEQ - 1, 0))

        @pl.loop(lo, hi)
        def _(i):
            r = pl.ds(_mo(kind * TOK + (i // 3) * SEQ, SEQ), SEQ)
            at = lax.rem(i, 3) * 128
            lanes, lanes2 = pl.ds(_mo(at, 128), 128), pl.ds(_mo(HALF + at, 128), 128)
            gate = PRE[lanes, r].astype(F32).T
            value = PRE[lanes2, r].astype(F32).T
            t0, t1, t2 = (tap[k : k + 1, lanes] for k in range(3))
            before, after = prev(gate), succ(gate)
            mixed = t0 * before + t1 * gate + t2 * after
            sig = jax.nn.sigmoid(mixed)
            active = mixed * sig
            ga = GA[r, lanes]
            hid[r, lanes] = (active * value).astype(BF)
            G[r, lanes2] = (ga * active).astype(BF)
            gm = ga * value * sig * (1.0 + mixed * (1.0 - sig))
            G[r, lanes] = (t1 * gm + t0 * succ(gm) + t2 * prev(gm)).astype(BF)
            for k, v in enumerate((before, gate, after)):
                tacc[k, :, lanes] += jnp.sum((gm * v).reshape(SEQ // 8, 8, 128), axis=0)

    def block(dst, left, right, zz, yy):
        at = _mo((zz * 2 + yy // 2) * FEAT, 128)
        dst[pl.ds(at, FEAT), :] = mm(left[:, pl.ds(at, FEAT)], right[...], 0, 0).astype(BF)

    def blocks(dst, left, right, yy, first):
        @pl.loop(0, 2)
        def _(k):
            zz = lax.rem(z + 2 - k + 4, 4) if first else lax.rem(z + 3 + k, 4)
            block(dst, left, right, zz, yy)

    def contrib(dst, cc, first, other=None):
        @pl.loop(0, 2)
        def _(i):
            k = 2 - i if first else lax.rem(3 + i, 4)
            at = _mo((lax.rem(x + k, 4) * 2 + cc) * FEAT, 128)
            term = mm(G[...], Wg[pl.ds(at, FEAT), :], 1, 1)
            if other is not None:
                term = term + other[k].astype(F32)
            dst[k] = term.astype(BF)

    pl.semaphore_wait(barrier, 13)
    for m in stats:
        m.start()
    gd.b0.m3.start()
    gd.lo.start()
    xo.d[0].start()
    xo.b.m0.start()
    gd.b0.m2.start()
    gd.u[0].start()
    xo.b.m1.start()
    gd.b0.m1.start()
    gd.b0.m0.start()
    own_lanes = pl.ds(_mo(tp * FEAT, 128), FEAT)
    X[0:TOK, own_lanes] = xin[...]
    gd.keep()
    split(taps, tap, None)
    tacc[...] = jnp.zeros_like(tacc)
    for m in loads[2:4]:
        m.wait()
    split(gatew, wgm.at[:, 0:HALF], wgt.at[:, 0:HALF])
    split(valuew, wgm.at[:, HALF : 2 * HALF], wgt.at[:, HALF : 2 * HALF])
    gw.keep()
    gw.b0.m1.start()
    gw.b0.m2.start()
    gw.b0.m3.start()
    gw.u[0].start()
    gw.b0.m0.start()
    sems.take(stats_j, st.at[pl.ds(1, 7)])
    tot = st[0]
    for k in range(1, 8):
        tot = tot + st[k]
    inverse = lax.rsqrt(tot[0:4] / D + EPSILON)
    coef = inverse * inverse * (tot[4:8] / D)

    def column(v):
        v = jnp.concatenate([jnp.broadcast_to(v[i : i + 1], (128, 128)).T for i in range(4)], axis=0)
        return jnp.concatenate([v, v, v], axis=1)

    inv = column(inverse)
    pf = pre[...].astype(F32)
    cf = cot[...].astype(F32)
    scaled = gain[...][None, :] * cf
    g = (inv * (scaled - pf * column(coef))).astype(BF)
    gpo[...] = g
    GP[0:TOK, own_lanes] = g
    small[...] = jnp.broadcast_to(jnp.sum(cf * pf * inv, axis=0, keepdims=True), (8, FEAT))
    go.lo[0].start()
    go.b.m3.start()
    go.lo[1].start()
    go.b.m1.start()
    go.b.m0.start()
    go.b.m2.start()
    go.d[0].start()
    gd.lo.wait_recv()
    gd.b1.m1.start()
    gd.b1.m3.start()
    gd.b1.m0.start()
    gd.b1.m2.start()
    gd.u4.start()
    gd.b0.f0()
    gw.lo.start()
    for m in loads[4:]:
        m.wait()
    split_rows(saved.at[0], PRE.at[0:HALF, 0:TOK], pt.at[0:HALF])
    split_rows(saved.at[1], PRE.at[HALF : 2 * HALF, 0:TOK], pt.at[HALF : 2 * HALF])

    gd.b0.f1()
    gd.n2()
    gd.n1()
    plo.start()
    xo.lo[0].start()
    xo.lo[1].start()
    gd.b1.f0()
    go.lo[0].wait_recv()
    gp.b.m3.start()
    gp.b.m0.start()
    gw.b0.f1()
    go.lo[1].wait_recv()
    gp.b.m2.start()
    gp.b.m1.start()
    gp.d[0].start()
    go.b.f1()
    go.n2()
    gd.u4.wait_recv()
    gd.b2.m3.start()
    gd.b2.m2.start()
    gd.b2.m1.start()
    gd.b2.m0.start()
    gw.u[0].wait_recv()
    gw.b3.m3.start()
    gw.b3.m1.start()
    gw.b3.m0.start()
    gw.b3.m2.start()
    gd.far()
    go.b.f0()
    gw.b0.f0()
    gd.b1.f1()
    gw.lo.wait_recv()
    gw.b1.m0.start()
    gw.b1.m1.start()
    gw.b1.m2.start()
    gw.u4.start()
    gw.b1.m3.start()
    gd.b2.f1()
    gw.b3.f1()
    gw.n2()
    go.n1()
    gp.b.f0()
    gp.b.f1()
    xo.b.m3.start()
    xo.b.m2.start()
    xo.b.f1()
    gw.n1()
    gd.b2.f0()
    gw.b3.f0()
    go.far()
    gw.u4.wait_recv()
    gw.b2.m1.start()
    gw.b2.m0.start()
    gw.b2.m2.start()
    gw.b2.m3.start()
    gp.n1()
    go.arrived()
    xo.b.f0()
    gw.b1.f0()
    gp.n2()
    gd.arrived()
    gp.far()
    gw.b1.f1()
    grad_act(0)
    middle(0, 0, 6)
    gp.arrived()
    gw.b2.f1()
    gw.b2.f0()
    gw.far()
    grad_act(1)
    xo.n1()
    middle(0, 6, 12)
    plo.wait_recv()
    middle(1, 0, 6)
    xo.lo[0].wait_recv()
    xp.b.m3.start()
    xp.b.m0.start()
    xo.n2()
    middle(1, 6, 12)
    xo.far()
    blocks(Dd, GP, hid, yh, True)
    sd.zq.m2.start()
    sd.zq.m1.start()
    sd.v[2].start()
    sd.v[1].start()
    sd.zq.m0.start()
    blocks(Dd, GP, hid, yh, False)
    sd.v[3].start()
    sd.zq.m3.start()
    sd.v[0].start()
    gw.arrived()
    xo.lo[1].wait_recv()
    xp.b.m2.start()
    xp.d[0].start()
    xp.b.m1.start()
    contrib(CS, sib, True)
    e[1].start()
    e[2].start()
    for k in range(3):
        small[k : k + 1, :] = jnp.sum(tacc[k], axis=0, keepdims=True)
    for m in sz_m:
        m.start()
    xp.b.f0()
    blocks(Dd, GP, hid, y, True)
    sd.zp.m0.start()
    sd.zp.m2.start()
    sd.zp.m1.start()
    contrib(CS, sib, False)
    e[3].start()
    e[0].start()
    sd.merge_hi(2)
    sd.zo.m0.start()
    sd.zo.m1.start()
    xp.b.f1()
    blocks(Dd, GP, hid, y, False)
    sd.zp.m3.start()
    xp.n1()
    sd.merge_hi(1)
    sd.zo.m2.start()
    sd.zq.g1()
    e[2].wait_recv()
    e[1].wait_recv()
    contrib(MC, c, True, E)
    xs.m0.start()
    xs.m2.start()
    xs.m1.start()
    sd.zp.g1()
    xp.n2()
    sd.zq.g0()
    sd.merge_hi(3)
    sd.zo.m3.start()
    sems.take(sz_j, sz)
    sy[3] = small[...] + sz[0] + sz[1] + sz[2]
    for m in sy_m:
        m.start()
    xp.far()
    e[3].wait_recv()
    e[0].wait_recv()
    contrib(MC, c, False, E)
    xs.m3.start()
    xo.arrived()
    sd.q(0)
    sd.q(1)
    sd.zp.g0()
    xp.arrived()
    blocks(Dg, X, G, yh, True)
    sw.zq.m2.start()
    sw.zh.m2.start()
    sw.v[1].start()
    sw.v[2].start()
    sw.zq.m1.start()
    sw.zh.m1.start()
    sw.zh.m0.start()
    sw.zq.m0.start()
    blocks(Dg, X, G, yh, False)
    sw.v[0].start()
    sw.v[3].start()
    sw.zh.m3.start()
    sw.zq.m3.start()
    blocks(Dg, X, G, y, True)
    sw.zp.m0.start()
    sw.zp.m1.start()
    sw.zb.m0.start()
    sw.zp.m2.start()
    sw.zb.m2.start()
    sw.zb.m1.start()
    xs.g0()
    xs.g1()
    blocks(Dg, X, G, y, False)
    sw.zp.m3.start()
    sw.zb.m3.start()
    sw.zq.g1()
    sd.p(0)
    sems.take(sy_j, sy.at[pl.ds(0, 3)])
    rest = gt_out.shape[1] - HALF
    mine_sum = sy[3] + sy[0]
    their_sum = sy[1] + sy[2]

    @pl.when(hs == 0)
    def _():
        gt_out[:, :HALF] = mine_sum[0:3]
        gt_out[:, HALF:] = their_sum[0:3, :rest]

    @pl.when(hs == 1)
    def _():
        gt_out[:, :HALF] = their_sum[0:3]
        gt_out[:, HALF:] = mine_sum[0:3, :rest]

    gn_out[...] = (mine_sum[3:4] + their_sum[3:4])[0]
    stores[4].start()
    stores[5].start()
    sd.zo.g0()
    sw.zh.g0()
    sw.zq.g0()
    sd.zo.g1()
    sw.zp.g1()
    sd.p(1)
    def put1(h, i, n, total):
        MC[0, pl.ds(_mo(TOK + i, 16), n), :] = total.astype(BF)

    xs.last(1, put1)
    xl.start()
    sd.merge_hi(0)

    sw.q(1)
    def put0(h, i, n, total):
        GA[pl.ds(_mo(i, 16), n), :] = total

    xs.last(0, put0)
    sw.merge_hi(2)
    sw.zo.m0.start()
    sw.zo.m1.start()
    sw.q(0)
    sw.zp.g0()
    sw.merge_hi(1)
    sw.zo.m2.start()
    sw.zh.g1()
    sw.merge_hi(3)
    sw.zo.m3.start()
    sw.p(1)
    sw.zb.g1()
    sd.t(1, (gd_out,))
    sw.zo.g1()
    sw.zo.g0()
    sw.p(0)
    sd.t(0, (gd_out,))
    sw.cross()
    sw.merge_hi(0)

    sw.zb.g0()
    sd.o(1, (gd_out,))
    sw.o(0, (gg_out, gv_out))
    sw.t(1, (gg_out, gv_out))
    sw.o(1, (gg_out, gv_out))
    sw.ob((gg_out, gv_out))
    xl.wait_recv()

    @pl.loop(0, 8)
    def _(i):
        r = pl.ds(_mo(i * 64, 16), 64)
        gi[r, :] = (GA[r, :] + xlin[r, :].astype(F32)).astype(BF)

    stores[0].start()
    sd.o(0, (gd_out,))
    stores[3].start()
    sw.t(0, (gg_out, gv_out))
    stores[1].start()
    stores[2].start()
    for m in stores:
        m.wait()
    sems.drain()


N, NS = 166, 20
VM = pl.BlockSpec(memory_space=pltpu.VMEM)
ANY = pl.BlockSpec(memory_space=pl.ANY)


def hand_on(*refs):
    src, dst, here = refs[:6], refs[6:12], refs[12:18]
    took = [pltpu.make_async_copy(a, b, refs[18].at[k]) for k, (a, b) in enumerate(zip(src, here))]
    gave = [pltpu.make_async_copy(a, b, refs[19].at[k]) for k, (a, b) in enumerate(zip(here, dst))]
    for m in took:
        m.start()
    for k in (1, 2, 3, 0, 4, 5):
        took[k].wait()
        gave[k].start()
    for m in gave:
        m.wait()


def on_device(
    inputs, cotangent, pre_norm, gate_pre, value_pre, gate_weight, value_weight, down_weight, conv_taps, norm_gain
):
    width = gate_pre.shape[1]

    def vm(*shape, dtype=BF):
        return pltpu.VMEM(shape, dtype)

    def wscratch(n):
        return [vm(3, 6, 96, n), vm(4, ROWS, n), vm(ROWS, n), vm(ROWS, n)]

    two = 2 * TOK
    outs = pl.pallas_call(
        kernel,
        out_shape=(
            jax.ShapeDtypeStruct((TOK, FEAT), BF),
            jax.ShapeDtypeStruct((ROWS, width), F32),
            jax.ShapeDtypeStruct((ROWS, width), F32),
            jax.ShapeDtypeStruct((ROWS, width), F32),
            jax.ShapeDtypeStruct((3, width), F32),
            jax.ShapeDtypeStruct((FEAT,), F32),
        ),
        in_specs=[VM] * 3 + [ANY] * 6 + [VM],
        out_specs=(ANY,) * 6,
        scratch_shapes=[
            vm(two, D), vm(two, D), vm(D, HALF), vm(D, 2 * HALF), vm(2 * HALF, two),
            vm(8, 8, 128, dtype=F32), vm(TOK, FEAT),
            vm(ROWS, HALF), vm(ROWS, HALF), vm(ROWS, 2 * HALF), vm(ROWS, 2 * HALF),
            vm(2 * HALF, TOK), vm(3, HALF, dtype=F32), vm(2, width, TOK), vm(2, 6, 16, 2 * HALF), vm(32, 2 * HALF),
            vm(TOK, FEAT), vm(ROWS, width), vm(ROWS, width), vm(ROWS, width),
            vm(TOK, FEAT), vm(ROWS, width, dtype=F32), vm(ROWS, width, dtype=F32), vm(ROWS, width, dtype=F32),
            vm(3, width, dtype=F32), vm(FEAT, dtype=F32),
            vm(two, HALF, dtype=F32), vm(two, HALF), vm(two, 2 * HALF), vm(3, 8, HALF, dtype=F32),
            vm(D, HALF), vm(D, 2 * HALF),
            vm(4, two, FEAT), vm(4, two, FEAT), vm(4, two, FEAT), vm(6, TOK, FEAT), vm(TOK, FEAT),
        ]
        + wscratch(HALF)
        + wscratch(2 * HALF)
        + [
            vm(8, FEAT, dtype=F32), vm(3, 8, FEAT, dtype=F32), vm(4, 8, FEAT, dtype=F32),
            pltpu.SemaphoreType.DMA((NS,)),
            pltpu.SemaphoreType.DMA((N,)),
            pltpu.SemaphoreType.DMA((12,)),
        ],
        compiler_params=pltpu.CompilerParams(
            collective_id=0, has_side_effects=True, vmem_limit_bytes=67043328
        ),
        name="layer",
    )(
        pre_norm, cotangent, norm_gain, inputs, down_weight.T,
        gate_weight, value_weight, gate_pre.T, value_pre.T, conv_taps,
    )
    outs = pl.pallas_call(
        hand_on,
        out_shape=tuple(jax.ShapeDtypeStruct(a.shape, a.dtype) for a in outs),
        in_specs=[ANY] * 6,
        out_specs=(ANY,) * 6,
        scratch_shapes=[pltpu.VMEM(a.shape, a.dtype) for a in outs]
        + [pltpu.SemaphoreType.DMA((6,)), pltpu.SemaphoreType.DMA((6,))],
        name="hand_on",
    )(*outs)
    gi, gg, gv, gd, gt, gn = outs
    return (gi, gg, gv, gd.T, gt, gn)


def solution(mesh):
    split = Mesh(mesh.devices.reshape(4, 4, 4, 2), ("z", "y", "x", "c"))
    fs, tp = ("z", "y"), ("x", "c")
    both, across = P(fs, tp), P(tp, fs)
    in_specs = (both, both, both, both, both, both, both, across, P(None, tp), P(tp))
    out_specs = (both, both, both, across, P(None, tp), P(tp))
    return jax.shard_map(on_device, mesh=split, in_specs=in_specs, out_specs=out_specs, check_vma=False)
```

```python
import jax
import jax.numpy as jnp
from jax import lax
from jax.experimental import pallas as pl
from jax.experimental.pallas import tpu as pltpu
from jax.sharding import Mesh
from jax.sharding import PartitionSpec as P

D = 3072
SEQ = 128
EPSILON = 1e-06
HALF = 384
ROWS = 192
TOK = 512
FEAT = 384
BF = jnp.bfloat16
F32 = jnp.float32
MESH = pl.DeviceIdType.MESH


def _mo(v, m):
    return pl.multiple_of(v, m)


class Sems:
    def __init__(self, send, recv, units):
        self.send, self.recv, self.units = send, recv, units
        self.n, self.k, self.open, self.groups = 0, 0, {}, []

    def _send(self, src):
        key, rows = src.shape[1:] if len(src.shape) == 2 else None, src.shape[0]
        if src.dtype == F32:
            key, rows = src.shape, 1
        if key not in self.units:
            self.groups.append([src, None])
            return len(self.groups) - 1
        ref, cap = self.units[key]
        at = self.open.get(key)
        if at is None or self.groups[at][1] + rows > cap:
            at = self.open[key] = len(self.groups)
            self.groups.append([ref, 0])
        self.groups[at][1] += rows
        return at

    def joint(self):
        self.n += 1
        return self.n - 1

    def msg(self, src, dst, share=None, **dev):
        return pltpu.make_async_remote_copy(
            src_ref=src,
            dst_ref=dst,
            send_sem=self.send.at[self._send(src)],
            recv_sem=self.recv.at[self.joint() if share is None else share],
            device_id=dev,
            device_id_type=MESH,
        )

    def take(self, share, ref):
        pltpu.make_async_copy(ref, ref, self.recv.at[share]).wait()

    def drain(self):
        assert len(self.groups) <= NS and self.n <= N
        for k, (ref, rows) in enumerate(self.groups):
            if rows is not None:
                ref = ref.at[pl.ds(0, rows)]
            pltpu.make_async_copy(ref, ref, self.send.at[k]).wait()


class Bcast:
    def __init__(self, sems, axis, me, own, slot, late=None):
        up, down = lax.rem(me + 1, 4), lax.rem(me + 3, 4)
        to_up, to_down = {axis: up}, {axis: down}
        self.m0 = sems.msg(own(0), slot(me, 0), **to_up)
        self.m1 = sems.msg(own(1), slot(me, 1), **to_down)
        self.m2 = sems.msg(own(1), slot(me, 1), late, **to_up)
        self.m3 = sems.msg(own(0), slot(me, 0), late, **to_down)
        self.m4 = sems.msg(slot(down, 0), slot(down, 0), late, **to_up)
        self.m5 = sems.msg(slot(up, 1), slot(up, 1), late, **to_down)

    def f0(self):
        self.m0.wait_recv()
        self.m4.start()

    def f1(self):
        self.m1.wait_recv()
        self.m5.start()

    def near(self):
        self.m2.wait_recv()
        self.m3.wait_recv()

    def far(self):
        self.m4.wait_recv()
        self.m5.wait_recv()


class Scatter:
    def __init__(self, sems, axis, me, chunk, got, rows, step):
        up, down = lax.rem(me + 1, 4), lax.rem(me + 3, 4)
        far = lax.rem(me + 2, 4)
        to_up, to_down = {axis: up}, {axis: down}
        self.me, self.up, self.down = me, up, down
        self.chunk, self.got, self.rows, self.step = chunk, got, rows, step
        self.m0 = sems.msg(chunk(far, 0), got.at[0], **to_up)
        self.m1 = sems.msg(chunk(far, 1), got.at[1], **to_down)
        self.m2 = sems.msg(chunk(up, 1), got.at[2], **to_up)
        self.m3 = sems.msg(chunk(down, 0), got.at[3], **to_down)
        self.m4 = sems.msg(chunk(up, 0), got.at[4], **to_up)
        self.m5 = sems.msg(chunk(down, 1), got.at[5], **to_down)

    def g0(self):
        self.m0.wait_recv()
        add_to(self.chunk(self.up, 0), self.got.at[0], self.rows, self.step)
        self.m4.start()

    def g1(self):
        self.m1.wait_recv()
        add_to(self.chunk(self.down, 1), self.got.at[1], self.rows, self.step)
        self.m5.start()

    def last(self, h, put):
        a, b = ((3, 4), (2, 5))[h]
        (self.m3, self.m2)[h].wait_recv()
        (self.m4, self.m5)[h].wait_recv()
        n = self.step
        own = self.chunk(self.me, h)

        @pl.loop(0, self.rows // n)
        def _(i):
            r = pl.ds(_mo(i * n, 16), n)
            put(h, i * n, n, own[r, :].astype(F32) + self.got[a, r, :].astype(F32) + self.got[b, r, :].astype(F32))


def add_to(dst, src, rows, step):
    @pl.loop(0, rows // step)
    def _(i):
        r = pl.ds(_mo(i * step, 16), step)
        dst[r, :] = (dst[r, :].astype(F32) + src[r, :].astype(F32)).astype(BF)


def mm(a, b, ca, cb):
    return lax.dot_general(a, b, (((ca,), (cb,)), ((), ())), preferred_element_type=F32)


def kernel(
    pre, cot, gain, xin_hbm, down_hbm, gatew_hbm, valuew_hbm, gatep, valuep, taps,
    *refs,
):
    results, scratch = refs[:6], refs[6:]
    (
        GP, X, Wd, Wg, PRE, st, gpo, wdm,
        wdt, wgm, wgt, pt, tap, saved, tgot, tin, xin, down,
        gatew, valuew, gi, gg_out, gv_out, gd_out, gt_out, gn_out,
        GA, hid, G, tacc, Dd, Dg, CS, MC,
        E, xgot, xlin, dgot, dhb, dhq, dlin, ggot,
        ghb, ghq, glin, small, sz, sy, ss, rs,
        ls,
    ) = scratch
    z, y = lax.axis_index("z"), lax.axis_index("y")
    x, c = lax.axis_index("x"), lax.axis_index("c")
    yp = y + 1 - 2 * lax.rem(y, 2)
    yh = 3 - y
    yq = yh + 1 - 2 * lax.rem(yh, 2)
    hs = lax.rem((y + 1) // 2, 2)
    sib = 1 - c
    tp = x * 2 + c
    zk = [lax.rem(z + k, 4) for k in range(4)]
    xk = [lax.rem(x + k, 4) for k in range(4)]
    units = {(HALF,): (Dd, D), (2 * HALF,): (Dg, D), (8, 128): (st, 8), (8, FEAT): (sz, 3)}
    sems = Sems(ss, rs, units)
    hbm = (down_hbm, xin_hbm, gatew_hbm, valuew_hbm, gatep, valuep)
    here = (down, xin, gatew, valuew, saved.at[0], saved.at[1])
    loads = [pltpu.make_async_copy(a, b, ls.at[k]) for k, (a, b) in enumerate(zip(hbm, here))]
    for m in loads:
        m.start()
    found = (gi, gg_out, gv_out, gd_out, gt_out, gn_out)
    stores = [pltpu.make_async_copy(a, b, ls.at[6 + k]) for k, (a, b) in enumerate(zip(found, results))]

    barrier = pltpu.get_barrier_semaphore()
    peers = [{"z": zk[1]}, {"z": zk[2]}, {"z": zk[3]}, {"y": yp}, {"y": yh}, {"y": yq}]
    tps = []
    for k in range(1, 8):
        t = lax.rem(tp + k, 8)
        tps.append({"x": t // 2, "c": lax.rem(t, 2)})
    for dev in peers + tps:
        pl.semaphore_signal(barrier, inc=1, device_id=dev, device_id_type=MESH)

    def lane_sums(v):
        v = v[:, :128] + v[:, 128:256] + v[:, 256:384]
        return jnp.sum(v.T, axis=0, keepdims=True)

    pf = pre[...].astype(F32)
    cf = cot[...].astype(F32)
    scaled = gain[...][None, :] * cf
    for j, v in enumerate((lane_sums(pf * pf), lane_sums(pf * scaled))):
        for i in range(4):
            st[0, j * 4 + i : j * 4 + i + 1, :] = v[:, i * 128 : (i + 1) * 128]

    def split(src, mine, theirs):
        n = src.shape[0]
        rest = src.shape[1] - HALF
        fill = jnp.zeros((n, HALF - rest), src.dtype)

        @pl.when(hs == 0)
        def _():
            mine[...] = src[:, :HALF]
            if theirs is not None:
                theirs[:, :rest] = src[:, HALF:]
                theirs[:, rest:] = fill

        @pl.when(hs == 1)
        def _():
            mine[:, :rest] = src[:, HALF:]
            mine[:, rest:] = fill
            if theirs is not None:
                theirs[...] = src[:, :HALF]

    loads[0].wait()
    split(down, wdm, wdt)
    loads[1].wait()

    def split_rows(src, mine, theirs):
        rest = src.shape[0] - HALF
        fill = jnp.zeros((HALF - rest, src.shape[1]), src.dtype)

        @pl.when(hs == 0)
        def _():
            mine[...] = src[:HALF]
            theirs[:rest] = src[HALF:]
            theirs[rest:] = fill

        @pl.when(hs == 1)
        def _():
            mine[:rest] = src[HALF:]
            mine[rest:] = fill
            theirs[...] = src[:HALF]

    class Gather:
        def __init__(self, mine, theirs, buf, tail=0):
            def rows(zz, yy, h=None):
                if h is None:
                    return buf.at[pl.ds(_mo((zz * 4 + yy) * ROWS, 16), ROWS)]
                return buf.at[pl.ds(_mo((zz * 4 + yy) * ROWS + h * 96, 16), 96)]

            self.b0 = Bcast(
                sems, "z", z, lambda h: mine.at[pl.ds(h * 96, 96)], lambda zz, h: rows(zz, y, h)
            )
            self.lo = sems.msg(theirs, rows(z, y), y=yp)
            zs = [zk[0], zk[3], zk[1], zk[2]]
            def front(zz, yy):
                return buf.at[pl.ds(_mo((zz * 4 + yy) * ROWS, 16), ROWS - tail)]

            def back(zz, yy, h):
                at = (zz * 4 + yy) * ROWS + ROWS - tail + h * (tail // 2)
                return buf.at[pl.ds(_mo(at, 16), tail // 2)]

            self.j = sems.joint()
            self.u = [sems.msg(mine, rows(z, y), None if tail else self.j, y=yh)]
            self.u += [sems.msg(front(zz, y), front(zz, y), self.j, y=yh) for zz in zs[1:]]
            self.due = 8 * 96 + 3 * (ROWS - tail) + (2 * tail if tail else ROWS)
            if tail:
                self.b3 = Bcast(sems, "z", z, lambda h: back(z, yh, h), lambda zz, h: back(zz, yh, h), self.j)
            self.u4 = sems.msg(rows(z, yp), rows(z, yp), y=yh)
            self.b1 = Bcast(sems, "z", z, lambda h: rows(z, yp, h), lambda zz, h: rows(zz, yp, h), self.j)
            self.b2 = Bcast(sems, "z", z, lambda h: rows(z, yq, h), lambda zz, h: rows(zz, yq, h), self.j)
            self.mine, self.buf, self.tail = mine, buf, tail

        def keep(self):
            self.buf[pl.ds(_mo((z * 4 + y) * ROWS, 16), ROWS), :] = self.mine[...]

        def n1(self):
            self.b0.m2.wait_recv()
            self.u[1].start()

        def n2(self):
            self.b0.m3.wait_recv()
            self.u[2].start()

        def far(self):
            self.b0.far()
            self.u[3].start()

        def arrived(self):
            sems.take(self.j, self.buf.at[pl.ds(0, self.due)])

    class Acts:
        def __init__(self, own, buf, kind):
            def slot(xx, h=None):
                lanes = pl.ds(_mo((xx * 2 + c) * FEAT, 128), FEAT)
                if h is None:
                    return buf.at[pl.ds(kind * TOK, TOK), lanes]
                return buf.at[pl.ds(kind * TOK + h * 256, 256), lanes]

            half = (lambda h: own.at[pl.ds(h * 256, 256)]) if kind == 0 else (lambda h: slot(x, h))
            self.b = Bcast(sems, "x", x, half, slot)
            xs = [xk[0], xk[3], xk[1], xk[2]]
            self.j = sems.joint()
            self.d = [
                sems.msg(own if (k == 0 and kind == 0) else slot(xx), slot(xx), self.j, c=sib)
                for k, xx in enumerate(xs)
            ]
            if kind == 0:
                lanes = pl.ds(_mo(tp * FEAT, 128), FEAT)
                self.lo = [
                    sems.msg(own.at[pl.ds(h * 256, 256)], buf.at[pl.ds(TOK + h * 256, 256), lanes], y=yp) for h in (0, 1)
                ]

        def n1(self):
            self.b.m2.wait_recv()
            self.d[1].start()

        def n2(self):
            self.b.m3.wait_recv()
            self.d[2].start()

        def far(self):
            self.b.far()
            self.d[3].start()

        def arrived(self):
            sems.take(self.j, Dd.at[pl.ds(0, 4 * TOK)])

    class Reduce:
        def __init__(self, src, got, hb, hq, lin, tail=0, tgot=None, tin=None):
            def rows(zz, yy, h=None):
                if h is None:
                    return src.at[pl.ds(_mo((zz * 4 + yy) * ROWS, 16), ROWS)]
                return src.at[pl.ds(_mo((zz * 4 + yy) * ROWS + h * 96, 16), 96)]

            self.rows, self.hb, self.hq, self.lin = rows, hb, hq, lin
            self.zq = Scatter(sems, "z", z, lambda zz, h: rows(zz, yq, h), got.at[0], 96, 48)
            self.zp = Scatter(sems, "z", z, lambda zz, h: rows(zz, yp, h), got.at[1], 96, 48)
            part = (ROWS - tail) // 2
            self.part = part

            def front(zz, yy, h):
                return src.at[pl.ds(_mo((zz * 4 + yy) * ROWS + h * part, 16), part)]

            def back(zz, yy, h):
                at = (zz * 4 + yy) * ROWS + ROWS - tail + h * (tail // 2)
                return src.at[pl.ds(_mo(at, 16), tail // 2)]

            self.zo = Scatter(
                sems, "z", z, lambda zz, h: front(zz, y, h), got.at[2, :, pl.ds(0, part)], part, 16 if tail else 48
            )
            if tail:
                self.zh = Scatter(sems, "z", z, lambda zz, h: back(zz, yh, h), tgot.at[0], tail // 2, 16)
                self.zb = Scatter(sems, "z", z, lambda zz, h: back(zz, y, h), tgot.at[1], tail // 2, 16)
                whole = src.at[pl.ds(_mo((z * 4 + yh) * ROWS + ROWS - tail, 16), tail)]
                self.x = sems.msg(whole, tin, y=yh)
                self.tin, self.tail = tin, tail
            keep = pl.ds(0, ROWS - tail)
            self.v = [sems.msg(rows(zk[k], yh).at[keep], hb.at[k, keep], y=yh) for k in range(4)]
            half = [pl.ds(0, 96), pl.ds(96, 96)]
            self.w = [sems.msg(rows(z, yq, h), hq.at[half[h]], y=yh) for h in (0, 1)]
            self.l = [sems.msg(rows(z, yp, h), lin.at[half[h]], y=yp) for h in (0, 1)]

        def merge_hi(self, k):
            self.v[k].wait_recv()
            add_to(self.rows(zk[k], y), self.hb.at[k], 2 * self.part, 32 if self.part % 48 else 48)

        def q(self, h):
            own = self.rows(z, yq)

            def put(h, i, n, total):
                own[pl.ds(_mo(h * 96 + i, 16), n), :] = total.astype(BF)

            self.zq.last(h, put)
            self.w[h].start()

        def p(self, h):
            self.w[h].wait_recv()
            own = self.rows(z, yp)

            def put(h, i, n, total):
                r = pl.ds(_mo(h * 96 + i, 16), n)
                own[r, :] = (total + self.hq[r, :].astype(F32)).astype(BF)

            self.zp.last(h, put)
            self.l[h].start()

        def o(self, h, outs):
            def put(h, i, n, total):
                write(outs, hs, h * self.part + i, n, total)

            self.zo.last(h, put)

        def cross(self):
            own = self.rows(z, yh)

            def put(h, i, n, total):
                own[pl.ds(_mo(ROWS - self.tail + h * (self.tail // 2) + i, 16), n), :] = total.astype(BF)

            self.zh.last(0, put)
            self.zh.last(1, put)
            self.x.start()

        def ob(self, outs):
            self.x.wait_recv()

            def put(h, i, n, total):
                at = h * (self.tail // 2) + i
                write(outs, hs, ROWS - self.tail + at, n, total + self.tin[pl.ds(_mo(at, 16), n), :].astype(F32))

            self.zb.last(0, put)
            self.zb.last(1, put)

        def t(self, h, outs):
            self.l[h].wait_recv()

            @pl.loop(0, 2)
            def _(i):
                at = _mo(h * 96 + i * 48, 16)
                write(outs, 1 - hs, at, 48, self.lin[pl.ds(at, 48), :].astype(F32))

    def write(outs, half, row, n, value):
        r = pl.ds(_mo(row, 16), n)
        for j, out in enumerate(outs):
            part = value[:, j * HALF : (j + 1) * HALF]
            rest = out.shape[1] - HALF

            @pl.when(half == 0)
            def _():
                out[r, :HALF] = part

            @pl.when(half == 1)
            def _():
                out[r, HALF:] = part[:, :rest]

    gd = Gather(wdm, wdt, Wd)
    gw = Gather(wgm, wgt, Wg, 32)
    go, gp = Acts(gpo, GP, 0), Acts(None, GP, 1)
    xo, xp = Acts(xin, X, 0), Acts(None, X, 1)
    plo = sems.msg(pt, PRE.at[:, pl.ds(TOK, TOK)], y=yp)
    stats_j, sz_j, sy_j = sems.joint(), sems.joint(), sems.joint()
    stats = [sems.msg(st.at[0], st.at[k], stats_j, **tps[k - 1]) for k in range(1, 8)]
    sd = Reduce(Dd, dgot, dhb, dhq, dlin)
    sw = Reduce(Dg, ggot, ghb, ghq, glin, 32, tgot, tin)
    e = [sems.msg(CS.at[k], E.at[k], c=sib) for k in range(4)]
    xs = Scatter(sems, "x", x, lambda xx, h: MC.at[lax.rem(xx - x + 4, 4), pl.ds(h * TOK, TOK)], xgot, TOK, 64)
    xl = sems.msg(MC.at[0, pl.ds(TOK, TOK)], xlin, y=yp)
    sz_m = [sems.msg(small, sz.at[k - 1], sz_j, z=zk[k]) for k in (1, 2, 3)]
    sy_m = [sems.msg(sy.at[3], sy.at[k], sy_j, y=yy) for k, yy in enumerate((yh, yp, yq))]

    def grad_act(kind):
        @pl.loop(0, 2)
        def _(i):
            r = pl.ds(_mo(kind * TOK + i * 256, 256), 256)
            GA[r, :] = mm(GP[r, :], Wd[...], 1, 0)

    def middle(kind, lo, hi):
        row = lax.broadcasted_iota(jnp.int32, (SEQ, 128), 0)

        def prev(v):
            return jnp.where(row == 0, 0.0, pltpu.roll(v, 1, 0))

        def succ(v):
            return jnp.where(row == SEQ - 1, 0.0, pltpu.roll(v, SEQ - 1, 0))

        @pl.loop(lo, hi)
        def _(i):
            r = pl.ds(_mo(kind * TOK + (i // 3) * SEQ, SEQ), SEQ)
            at = lax.rem(i, 3) * 128
            lanes, lanes2 = pl.ds(_mo(at, 128), 128), pl.ds(_mo(HALF + at, 128), 128)
            gate = PRE[lanes, r].astype(F32).T
            value = PRE[lanes2, r].astype(F32).T
            t0, t1, t2 = (tap[k : k + 1, lanes] for k in range(3))
            before, after = prev(gate), succ(gate)
            mixed = t0 * before + t1 * gate + t2 * after
            sig = jax.nn.sigmoid(mixed)
            active = mixed * sig
            ga = GA[r, lanes]
            hid[r, lanes] = (active * value).astype(BF)
            G[r, lanes2] = (ga * active).astype(BF)
            gm = ga * value * sig * (1.0 + mixed * (1.0 - sig))
            G[r, lanes] = (t1 * gm + t0 * succ(gm) + t2 * prev(gm)).astype(BF)
            for k, v in enumerate((before, gate, after)):
                tacc[k, :, lanes] += jnp.sum((gm * v).reshape(SEQ // 8, 8, 128), axis=0)

    def block(dst, left, right, zz, yy):
        at = _mo((zz * 2 + yy // 2) * FEAT, 128)
        dst[pl.ds(at, FEAT), :] = mm(left[:, pl.ds(at, FEAT)], right[...], 0, 0).astype(BF)

    def blocks(dst, left, right, yy, first):
        @pl.loop(0, 2)
        def _(k):
            zz = lax.rem(z + 2 - k + 4, 4) if first else lax.rem(z + 3 + k, 4)
            block(dst, left, right, zz, yy)

    def contrib(dst, cc, first, other=None):
        @pl.loop(0, 2)
        def _(i):
            k = 2 - i if first else lax.rem(3 + i, 4)
            at = _mo((lax.rem(x + k, 4) * 2 + cc) * FEAT, 128)
            term = mm(G[...], Wg[pl.ds(at, FEAT), :], 1, 1)
            if other is not None:
                term = term + other[k].astype(F32)
            dst[k] = term.astype(BF)

    pl.semaphore_wait(barrier, 13)
    for m in stats:
        m.start()
    gd.b0.m3.start()
    gd.lo.start()
    xo.d[0].start()
    xo.b.m0.start()
    gd.b0.m2.start()
    gd.u[0].start()
    xo.b.m1.start()
    gd.b0.m1.start()
    gd.b0.m0.start()
    own_lanes = pl.ds(_mo(tp * FEAT, 128), FEAT)
    X[0:TOK, own_lanes] = xin[...]
    gd.keep()
    split(taps, tap, None)
    tacc[...] = jnp.zeros_like(tacc)
    for m in loads[2:4]:
        m.wait()
    split(gatew, wgm.at[:, 0:HALF], wgt.at[:, 0:HALF])
    split(valuew, wgm.at[:, HALF : 2 * HALF], wgt.at[:, HALF : 2 * HALF])
    gw.keep()
    gw.b0.m1.start()
    gw.b0.m2.start()
    gw.b0.m3.start()
    gw.u[0].start()
    gw.b0.m0.start()
    sems.take(stats_j, st.at[pl.ds(1, 7)])
    tot = st[0]
    for k in range(1, 8):
        tot = tot + st[k]
    inverse = lax.rsqrt(tot[0:4] / D + EPSILON)
    coef = inverse * inverse * (tot[4:8] / D)

    def column(v):
        v = jnp.concatenate([jnp.broadcast_to(v[i : i + 1], (128, 128)).T for i in range(4)], axis=0)
        return jnp.concatenate([v, v, v], axis=1)

    inv = column(inverse)
    pf = pre[...].astype(F32)
    cf = cot[...].astype(F32)
    scaled = gain[...][None, :] * cf
    g = (inv * (scaled - pf * column(coef))).astype(BF)
    gpo[...] = g
    GP[0:TOK, own_lanes] = g
    small[...] = jnp.broadcast_to(jnp.sum(cf * pf * inv, axis=0, keepdims=True), (8, FEAT))
    go.lo[0].start()
    go.b.m3.start()
    go.lo[1].start()
    go.b.m1.start()
    go.b.m0.start()
    go.b.m2.start()
    go.d[0].start()
    gd.lo.wait_recv()
    gd.b1.m1.start()
    gd.b1.m3.start()
    gd.b1.m0.start()
    gd.b1.m2.start()
    gd.u4.start()
    gd.b0.f0()
    gw.lo.start()
    for m in loads[4:]:
        m.wait()
    split_rows(saved.at[0], PRE.at[0:HALF, 0:TOK], pt.at[0:HALF])
    split_rows(saved.at[1], PRE.at[HALF : 2 * HALF, 0:TOK], pt.at[HALF : 2 * HALF])

    gd.b0.f1()
    gd.n2()
    gd.n1()
    plo.start()
    xo.lo[0].start()
    xo.lo[1].start()
    gd.b1.f0()
    go.lo[0].wait_recv()
    gp.b.m3.start()
    gp.b.m0.start()
    gw.b0.f1()
    go.lo[1].wait_recv()
    gp.b.m2.start()
    gp.b.m1.start()
    gp.d[0].start()
    go.b.f1()
    go.n2()
    gd.u4.wait_recv()
    gd.b2.m3.start()
    gd.b2.m2.start()
    gd.b2.m1.start()
    gd.b2.m0.start()
    gw.u[0].wait_recv()
    gw.b3.m3.start()
    gw.b3.m1.start()
    gw.b3.m0.start()
    gw.b3.m2.start()
    gd.far()
    go.b.f0()
    gw.b0.f0()
    gd.b1.f1()
    gw.lo.wait_recv()
    gw.b1.m0.start()
    gw.b1.m1.start()
    gw.b1.m2.start()
    gw.u4.start()
    gw.b1.m3.start()
    gd.b2.f1()
    gw.b3.f1()
    gw.n2()
    go.n1()
    gp.b.f0()
    gp.b.f1()
    xo.b.m3.start()
    xo.b.m2.start()
    xo.b.f1()
    gw.n1()
    gd.b2.f0()
    gw.b3.f0()
    go.far()
    gw.u4.wait_recv()
    gw.b2.m1.start()
    gw.b2.m0.start()
    gw.b2.m2.start()
    gw.b2.m3.start()
    gp.n1()
    go.arrived()
    xo.b.f0()
    gw.b1.f0()
    gp.n2()
    gd.arrived()
    gp.far()
    gw.b1.f1()
    grad_act(0)
    middle(0, 0, 6)
    gp.arrived()
    gw.b2.f1()
    gw.b2.f0()
    gw.far()
    grad_act(1)
    xo.n1()
    middle(0, 6, 12)
    plo.wait_recv()
    middle(1, 0, 6)
    xo.lo[0].wait_recv()
    xp.b.m3.start()
    xp.b.m0.start()
    xo.n2()
    middle(1, 6, 12)
    xo.far()
    blocks(Dd, GP, hid, yh, True)
    sd.zq.m2.start()
    sd.zq.m1.start()
    sd.v[2].start()
    sd.v[1].start()
    sd.zq.m0.start()
    blocks(Dd, GP, hid, yh, False)
    sd.v[3].start()
    sd.zq.m3.start()
    sd.v[0].start()
    gw.arrived()
    xo.lo[1].wait_recv()
    xp.b.m2.start()
    xp.d[0].start()
    xp.b.m1.start()
    contrib(CS, sib, True)
    e[1].start()
    e[2].start()
    for k in range(3):
        small[k : k + 1, :] = jnp.sum(tacc[k], axis=0, keepdims=True)
    for m in sz_m:
        m.start()
    xp.b.f0()
    blocks(Dd, GP, hid, y, True)
    sd.zp.m0.start()
    sd.zp.m2.start()
    sd.zp.m1.start()
    contrib(CS, sib, False)
    e[3].start()
    e[0].start()
    sd.merge_hi(2)
    sd.zo.m0.start()
    sd.zo.m1.start()
    xp.b.f1()
    blocks(Dd, GP, hid, y, False)
    sd.zp.m3.start()
    xp.n1()
    sd.merge_hi(1)
    sd.zo.m2.start()
    sd.zq.g1()
    e[2].wait_recv()
    e[1].wait_recv()
    contrib(MC, c, True, E)
    xs.m0.start()
    xs.m2.start()
    xs.m1.start()
    sd.zp.g1()
    xp.n2()
    sd.zq.g0()
    sd.merge_hi(3)
    sd.zo.m3.start()
    sems.take(sz_j, sz)
    sy[3] = small[...] + sz[0] + sz[1] + sz[2]
    for m in sy_m:
        m.start()
    xp.far()
    e[3].wait_recv()
    e[0].wait_recv()
    contrib(MC, c, False, E)
    xs.m3.start()
    xo.arrived()
    sd.q(0)
    sd.q(1)
    sd.zp.g0()
    xp.arrived()
    blocks(Dg, X, G, yh, True)
    sw.zq.m2.start()
    sw.zh.m2.start()
    sw.v[1].start()
    sw.v[2].start()
    sw.zq.m1.start()
    sw.zh.m1.start()
    sw.zh.m0.start()
    sw.zq.m0.start()
    blocks(Dg, X, G, yh, False)
    sw.v[0].start()
    sw.v[3].start()
    sw.zh.m3.start()
    sw.zq.m3.start()
    blocks(Dg, X, G, y, True)
    sw.zp.m0.start()
    sw.zp.m1.start()
    sw.zb.m0.start()
    sw.zp.m2.start()
    sw.zb.m2.start()
    sw.zb.m1.start()
    xs.g0()
    xs.g1()
    blocks(Dg, X, G, y, False)
    sw.zp.m3.start()
    sw.zb.m3.start()
    sw.zq.g1()
    sd.p(0)
    sems.take(sy_j, sy.at[pl.ds(0, 3)])
    rest = gt_out.shape[1] - HALF
    mine_sum = sy[3] + sy[0]
    their_sum = sy[1] + sy[2]

    @pl.when(hs == 0)
    def _():
        gt_out[:, :HALF] = mine_sum[0:3]
        gt_out[:, HALF:] = their_sum[0:3, :rest]

    @pl.when(hs == 1)
    def _():
        gt_out[:, :HALF] = their_sum[0:3]
        gt_out[:, HALF:] = mine_sum[0:3, :rest]

    gn_out[...] = (mine_sum[3:4] + their_sum[3:4])[0]
    stores[4].start()
    stores[5].start()
    sd.zo.g0()
    sw.zh.g0()
    sw.zq.g0()
    sd.zo.g1()
    sw.zp.g1()
    sd.p(1)
    def put1(h, i, n, total):
        MC[0, pl.ds(_mo(TOK + i, 16), n), :] = total.astype(BF)

    xs.last(1, put1)
    xl.start()
    sd.merge_hi(0)

    sw.q(1)
    def put0(h, i, n, total):
        GA[pl.ds(_mo(i, 16), n), :] = total

    xs.last(0, put0)
    sw.merge_hi(2)
    sw.zo.m0.start()
    sw.zo.m1.start()
    sw.q(0)
    sw.zp.g0()
    sw.merge_hi(1)
    sw.zo.m2.start()
    sw.zh.g1()
    sw.merge_hi(3)
    sw.zo.m3.start()
    sw.p(1)
    sw.zb.g1()
    sd.t(1, (gd_out,))
    sw.zo.g1()
    sw.zo.g0()
    sw.p(0)
    sd.t(0, (gd_out,))
    sw.cross()
    sw.merge_hi(0)

    sw.zb.g0()
    sd.o(1, (gd_out,))
    sw.o(0, (gg_out, gv_out))
    sw.t(1, (gg_out, gv_out))
    sw.o(1, (gg_out, gv_out))
    sw.ob((gg_out, gv_out))
    xl.wait_recv()

    @pl.loop(0, 8)
    def _(i):
        r = pl.ds(_mo(i * 64, 16), 64)
        gi[r, :] = (GA[r, :] + xlin[r, :].astype(F32)).astype(BF)

    stores[0].start()
    sd.o(0, (gd_out,))
    stores[3].start()
    sw.t(0, (gg_out, gv_out))
    stores[1].start()
    stores[2].start()
    for m in stores:
        m.wait()
    sems.drain()


N, NS = 143, 20
VM = pl.BlockSpec(memory_space=pltpu.VMEM)
ANY = pl.BlockSpec(memory_space=pl.ANY)


def hand_on(*refs):
    src, dst, here = refs[:6], refs[6:12], refs[12:18]
    took = [pltpu.make_async_copy(a, b, refs[18].at[k]) for k, (a, b) in enumerate(zip(src, here))]
    gave = [pltpu.make_async_copy(a, b, refs[19].at[k]) for k, (a, b) in enumerate(zip(here, dst))]
    for m in took:
        m.start()
    for k in (1, 2, 3, 0, 4, 5):
        took[k].wait()
        gave[k].start()
    for m in gave:
        m.wait()


def on_device(
    inputs, cotangent, pre_norm, gate_pre, value_pre, gate_weight, value_weight, down_weight, conv_taps, norm_gain
):
    width = gate_pre.shape[1]

    def vm(*shape, dtype=BF):
        return pltpu.VMEM(shape, dtype)

    def wscratch(n):
        return [vm(3, 6, 96, n), vm(4, ROWS, n), vm(ROWS, n), vm(ROWS, n)]

    two = 2 * TOK
    outs = pl.pallas_call(
        kernel,
        out_shape=(
            jax.ShapeDtypeStruct((TOK, FEAT), BF),
            jax.ShapeDtypeStruct((ROWS, width), F32),
            jax.ShapeDtypeStruct((ROWS, width), F32),
            jax.ShapeDtypeStruct((ROWS, width), F32),
            jax.ShapeDtypeStruct((3, width), F32),
            jax.ShapeDtypeStruct((FEAT,), F32),
        ),
        in_specs=[VM] * 3 + [ANY] * 6 + [VM],
        out_specs=(ANY,) * 6,
        scratch_shapes=[
            vm(two, D), vm(two, D), vm(D, HALF), vm(D, 2 * HALF), vm(2 * HALF, two),
            vm(8, 8, 128, dtype=F32), vm(TOK, FEAT),
            vm(ROWS, HALF), vm(ROWS, HALF), vm(ROWS, 2 * HALF), vm(ROWS, 2 * HALF),
            vm(2 * HALF, TOK), vm(3, HALF, dtype=F32), vm(2, width, TOK), vm(2, 6, 16, 2 * HALF), vm(32, 2 * HALF),
            vm(TOK, FEAT), vm(ROWS, width), vm(ROWS, width), vm(ROWS, width),
            vm(TOK, FEAT), vm(ROWS, width, dtype=F32), vm(ROWS, width, dtype=F32), vm(ROWS, width, dtype=F32),
            vm(3, width, dtype=F32), vm(FEAT, dtype=F32),
            vm(two, HALF, dtype=F32), vm(two, HALF), vm(two, 2 * HALF), vm(3, 8, HALF, dtype=F32),
            vm(D, HALF), vm(D, 2 * HALF),
            vm(4, two, FEAT), vm(4, two, FEAT), vm(4, two, FEAT), vm(6, TOK, FEAT), vm(TOK, FEAT),
        ]
        + wscratch(HALF)
        + wscratch(2 * HALF)
        + [
            vm(8, FEAT, dtype=F32), vm(3, 8, FEAT, dtype=F32), vm(4, 8, FEAT, dtype=F32),
            pltpu.SemaphoreType.DMA((NS,)),
            pltpu.SemaphoreType.DMA((N,)),
            pltpu.SemaphoreType.DMA((12,)),
        ],
        compiler_params=pltpu.CompilerParams(
            collective_id=0, has_side_effects=True, vmem_limit_bytes=67043328
        ),
        name="layer",
    )(
        pre_norm, cotangent, norm_gain, inputs, down_weight.T,
        gate_weight, value_weight, gate_pre.T, value_pre.T, conv_taps,
    )
    outs = pl.pallas_call(
        hand_on,
        out_shape=tuple(jax.ShapeDtypeStruct(a.shape, a.dtype) for a in outs),
        in_specs=[ANY] * 6,
        out_specs=(ANY,) * 6,
        scratch_shapes=[pltpu.VMEM(a.shape, a.dtype) for a in outs]
        + [pltpu.SemaphoreType.DMA((6,)), pltpu.SemaphoreType.DMA((6,))],
        name="hand_on",
    )(*outs)
    gi, gg, gv, gd, gt, gn = outs
    return (gi, gg, gv, gd.T, gt, gn)


def solution(mesh):
    split = Mesh(mesh.devices.reshape(4, 4, 4, 2), ("z", "y", "x", "c"))
    fs, tp = ("z", "y"), ("x", "c")
    both, across = P(fs, tp), P(tp, fs)
    in_specs = (both, both, both, both, both, both, both, across, P(None, tp), P(tp))
    out_specs = (both, both, both, across, P(None, tp), P(tp))
    return jax.shard_map(on_device, mesh=split, in_specs=in_specs, out_specs=out_specs, check_vma=False)
```
